256 devices in a mesh: grp: 2 (over y), kv: 32 (over z, core), tp: 4 (over x).
Axes of the slice: x: 4, y: 2, z: 16, core: 2. Of those that a mesh axis runs over, the one named last changes fastest.
The devices are a block of a 4x16x16 slice.
Arguments:
- tokens: bfloat16 [16, 16, 4096], P('grp'), parts along dimension 0, may hold values from -6 to 6
- norm_gain: bfloat16 [4096], replicated, may hold values from 0.099609375 to 1.8984375
- query_weight: bfloat16 [4096, 4096], P('kv', 'tp'), may hold values from -0.09375 to 0.09375
- key_weight: bfloat16 [4096, 1024], P('kv', 'tp'), may hold values from -0.15625 to 0.15625
- value_weight: bfloat16 [4096, 1024], P('kv', 'tp'), may hold values from -0.09375 to 0.09375
- out_weight: bfloat16 [4096, 4096], P(None, 'kv'), may hold values from -0.09375 to 0.09375
- head_gain: bfloat16 [128], replicated, may hold values from 0.099609375 to 1.8984375
- mix_lambda: float32 [32], P('tp'), may hold values from 0.3 to 0.8
- cache_keys: bfloat16 [16, 8, 16384, 128], P('grp', 'tp', 'kv'), parts along dimension 0, may hold values from -310 to 310
- cache_values: bfloat16 [16, 8, 16384, 128], P('grp', 'tp', 'kv'), parts along dimension 0, may hold values from -6 to 6
- lengths: int32 [16], P('grp'), parts along dimension 0, may hold values from 8192 to 16360, as said below
- accepted: int32 [16], P('grp'), parts along dimension 0, may hold values from 0 to 8
- parents: int32 [16, 16], P('grp'), parts along dimension 0, may hold values from 0 to 15, as said below
Outputs:
- mixed: bfloat16 [16, 16, 4096], P('grp', None, 'kv'), parts along dimension 0
- keys_out: bfloat16 [16, 8, 16384, 128], P('grp', 'tp', 'kv'), parts along dimension 0
- values_out: bfloat16 [16, 8, 16384, 128], P('grp', 'tp', 'kv'), parts along dimension 0
The draws below stay inside these ranges and needn't reach their ends.
There are 2 independent parts, one for each index of `grp`. The reference program is written for one: setup_inputs(seed, part) draws one part's arguments, and reference() takes and returns one part's arrays. A program takes and returns all parts, laid end to end along the dimension named above; an argument that names none is the same for every part. Nothing has to cross between parts.
Inputs may be any that keep to these rules, and one draw needn't show every extreme that they name: `lengths`: one sequence has exactly the largest length in every draw. `parents`: proposal 0 is the root and names itself; every other proposal i names one of 0 to i - 1.
All inputs are finite; a program needn't handle non-finite values.
Results may differ from the reference program's by a relative error of at most 0.014.
The reference program's roundings to bfloat16 on the way count: a program that leaves them out, or rounds other values in their place, can miss the bound.
Values may be sent and summed in bfloat16 or wider, within the bound.
No kernel may reach another device: no remote copies, remote signals or barrier semaphores. Data moves between devices by JAX's collectives and lax.ppermute only.
A program may use at most 128 MiB of HBM per device.

```python
import jax
import jax.numpy as jnp
from jax import lax

D = 4096
HEADS = 32
KV_HEADS = 8
QK_DIM = 64
V_DIM = 128
PROPOSALS = 16
SEQS = 8
CTX = 16384
N_KV = 32


def draw_cache_keys(key, part):
    shape = (SEQS, KV_HEADS, CTX, 2 * QK_DIM)
    first_key = jax.random.fold_in(jax.random.fold_in(key, 7), 0)
    drawn = 1.75 * jnp.clip(jax.random.normal(first_key, shape, jnp.float32), -6.0, 6.0)
    return drawn.astype(jnp.bfloat16)


def draw_lengths(key, part):
    first_key, second_key = jax.random.split(jax.random.fold_in(key, 11))
    longest = CTX - PROPOSALS - PROPOSALS // 2
    drawn = jax.random.randint(first_key, (SEQS,), CTX // 2, longest + 1)
    chosen = jax.random.randint(second_key, (), 0, SEQS)
    return jnp.where(jnp.arange(SEQS) == chosen, longest, drawn).astype(jnp.int32)


def draw_parents(key, part):
    upper = jnp.maximum(jnp.arange(PROPOSALS), 1)
    drawn = jax.random.randint(jax.random.fold_in(key, 13), (SEQS, PROPOSALS), 0, upper[None, :])
    return drawn.astype(jnp.int32)


def with_ends(entries, stream_key, least, top_value):
    longest = entries.shape.index(max(entries.shape))
    spots = []
    for shift in (0, 1):
        where = [jax.random.randint(jax.random.fold_in(stream_key, axis), (), 0, length) for axis, length in enumerate(entries.shape)]
        where[longest] = (where[longest] + shift) % entries.shape[longest]
        spots.append(tuple(where))
    return entries.at[spots[0]].set(least).at[spots[1]].set(top_value)


def steps_of(own_key, extent, cuts, smallest, high):
    level = 1.0
    for axis_at, shards_of in cuts:
        draws = jax.random.uniform(jax.random.fold_in(jax.random.fold_in(own_key, 6), axis_at), (shards_of,), jnp.float32, smallest / len(cuts), high / len(cuts))
        level = level * jnp.repeat(jnp.exp(draws), extent[axis_at] // shards_of).reshape((-1,) + (1,) * (len(extent) - 1 - axis_at))
    return level


def scatter_about(own_key, dims, deviation, most, cuts=(), kind=jnp.bfloat16):
    entries = jax.random.normal(own_key, dims, jnp.float32) * deviation
    if len(cuts) > 0:
        entries = steps_of(own_key, dims, cuts, -0.22, 0.18) * entries
    return jnp.clip(entries, min=-most, max=most).astype(kind)


def setup_inputs(seed: int = 0, part: int = 0) -> dict:
    streams_of = jax.random.split(jax.random.key(seed), 14)
    part_keys = jax.random.split(jax.random.fold_in(streams_of[13], part), 14)
    return {
        "tokens": scatter_about(part_keys[0], (SEQS, PROPOSALS, D), 1.0, 6.0),
        "norm_gain": jnp.clip(1.0 + 0.18 * jax.random.normal(streams_of[1], (D,), jnp.float32), 0.099609375, 1.8984375).astype(jnp.bfloat16),
        "query_weight": scatter_about(streams_of[2], (D, 2 * HEADS * QK_DIM), D ** -0.5, 0.09375, ((0, 32), (1, 4))),
        "key_weight": scatter_about(streams_of[3], (D, 2 * KV_HEADS * QK_DIM), (D // 3) ** -0.5, 0.15625, ((0, 32), (1, 4))),
        "value_weight": scatter_about(streams_of[4], (D, KV_HEADS * V_DIM), D ** -0.5, 0.09375, ((0, 32), (1, 4))),
        "out_weight": scatter_about(streams_of[5], (HEADS * V_DIM, D), (HEADS * V_DIM) ** -0.5, 0.09375, ((1, 32),)),
        "head_gain": jnp.clip(1.0 + 0.18 * jax.random.normal(streams_of[6], (V_DIM,), jnp.float32), 0.099609375, 1.8984375).astype(jnp.bfloat16),
        "mix_lambda": jnp.clip(0.3 + 0.5 * jax.random.uniform(streams_of[7], (HEADS,), jnp.float32) ** steps_of(streams_of[7], (HEADS,), ((0, 4),), -0.2, 0.2), 0.3, 0.8),
        "cache_keys": draw_cache_keys(jax.random.fold_in(jax.random.fold_in(streams_of[13], part), 71), part),
        "cache_values": scatter_about(part_keys[9], (SEQS, KV_HEADS, CTX, V_DIM), 1.0, 6.0, ((1, 4), (2, 32))),
        "lengths": draw_lengths(jax.random.fold_in(jax.random.fold_in(streams_of[13], part), 71), part),
        "accepted": with_ends(jax.random.randint(part_keys[11], (SEQS,), 0, PROPOSALS // 2 + 1), jax.random.fold_in(part_keys[11], 1), 0, (PROPOSALS // 2 + 1) - 1).astype(jnp.int32),
        "parents": draw_parents(jax.random.fold_in(jax.random.fold_in(streams_of[13], part), 71), part),
    }


NEG_FILL = -1e+30
ROTARY_BASE = 10000.0
NORM_EPS = 1e-06

def ancestry(parents):
    proposals = parents.shape[-1]
    indices = jnp.arange(proposals, dtype=jnp.int32)
    linked = (parents[:, :, None] == indices[None, None, :]) & (indices[None, :, None] > 0)
    reach = jnp.minimum(linked.astype(jnp.float32) + jnp.eye(proposals, dtype=jnp.float32)[None], 1.0)
    for squaring in range(proposals.bit_length()):
        reach = jnp.minimum(jnp.einsum('bij,bjk->bik', reach, reach), 1.0)
    return reach

def rotate(vectors, positions):
    half_dim = vectors.shape[-1] // 2
    inverse = ROTARY_BASE ** (-jnp.arange(half_dim, dtype=jnp.float32) / half_dim)
    angles = positions.astype(jnp.float32)[..., None, None] * inverse
    cosine = jnp.cos(angles)
    sine_part = jnp.sin(angles)
    first_half = vectors[..., :half_dim]
    second_half = vectors[..., half_dim:]
    return jnp.concatenate([first_half * cosine - second_half * sine_part, second_half * cosine + first_half * sine_part], axis=-1)

def block_mask(reach, starts, offset, span_len, proposals):
    positions = offset + jnp.arange(span_len, dtype=jnp.int32)
    relative = positions[None, :] - starts[:, None]
    slots = (relative[:, :, None] == jnp.arange(proposals, dtype=jnp.int32)[None, None, :]).astype(jnp.float32)
    in_tree = jnp.einsum('bij,bsj->bis', reach, slots) > 0.5
    return (relative < 0)[:, None, :] | in_tree

def block_partials(query_maps, block_keys, block_values, allowed):
    qk_dim = query_maps.shape[-1]
    highs, totals, sums = ([], [], [])
    for which in range(2):
        key_map = block_keys[..., which * qk_dim:(which + 1) * qk_dim]
        scores = jnp.einsum('bgrpd,bgsd->bgrps', query_maps[which].astype(jnp.float32), key_map.astype(jnp.float32)) * qk_dim ** (-0.5)
        scores = jnp.where(allowed[:, None, None], scores, NEG_FILL)
        highest = lax.optimization_barrier(jnp.max(scores, axis=-1))
        weights = jnp.where(allowed[:, None, None], jnp.exp(scores - highest[..., None]), 0.0)
        highs.append(highest)
        totals.append(lax.optimization_barrier(jnp.sum(weights, axis=-1)))
        rounded = weights.astype(jnp.bfloat16).astype(jnp.float32)
        sums.append(jnp.einsum('bgrps,bgsv->bgrpv', rounded, block_values.astype(jnp.float32)).astype(jnp.bfloat16))
    return (jnp.stack(highs), jnp.stack(totals), jnp.stack(sums))

def absorb(carry, pieces, first_index):
    highest, total_sum, acc_sum = carry
    piece_high, piece_total, piece_acc = pieces
    new_high = jnp.maximum(highest, lax.optimization_barrier(jnp.max(piece_high, axis=0)))
    scaling = jnp.exp(piece_high - new_high[None])
    keep_old = jnp.exp(highest - new_high)
    new_total = total_sum * keep_old + lax.optimization_barrier(jnp.sum(piece_total * scaling, axis=0))
    new_acc = acc_sum * keep_old[..., None] + lax.optimization_barrier(jnp.sum(piece_acc.astype(jnp.float32) * scaling[..., None], axis=0))
    return (new_high, new_total, new_acc)

def place_rows(cache_rows, fresh_rows, at_pos):
    zero = jnp.zeros((), jnp.int32)
    return lax.dynamic_update_slice(cache_rows, fresh_rows, (zero, at_pos.astype(jnp.int32), zero))

def reference(tokens, norm_gain, query_weight, key_weight, value_weight, out_weight, head_gain, mix_lambda, cache_keys, cache_values, lengths, accepted, parents):
    seqs, proposals, width = tokens.shape
    heads = mix_lambda.shape[0]
    kv_heads = cache_keys.shape[1]
    group = heads // kv_heads
    context = cache_keys.shape[2]
    qk_dim = cache_keys.shape[-1] // 2
    v_dim = cache_values.shape[-1]
    span_len = context // N_KV
    floats = tokens.astype(jnp.float32)
    normed = (floats * lax.rsqrt(lax.optimization_barrier(jnp.mean(floats * floats, axis=-1, keepdims=True)) + NORM_EPS) * norm_gain.astype(jnp.float32)).astype(jnp.bfloat16)
    rows = normed.reshape(seqs * proposals, width)
    reach = ancestry(parents)
    depth = (lax.optimization_barrier(jnp.sum(reach, axis=-1)) - 1.0).astype(jnp.int32)
    starts = lengths + accepted
    position = starts[:, None] + depth
    queries = jnp.dot(rows, query_weight, preferred_element_type=jnp.float32).reshape(seqs, proposals, heads * 2, qk_dim)
    queries = rotate(queries, position).astype(jnp.bfloat16)
    fresh_keys = jnp.dot(rows, key_weight, preferred_element_type=jnp.float32).reshape(seqs, proposals, kv_heads * 2, qk_dim)
    fresh_keys = rotate(fresh_keys, position).astype(jnp.bfloat16)
    fresh_values = jnp.dot(rows, value_weight, preferred_element_type=jnp.float32).astype(jnp.bfloat16)
    key_rows = jnp.transpose(fresh_keys.reshape(seqs, proposals, kv_heads, 2 * qk_dim), (0, 2, 1, 3))
    value_rows = jnp.transpose(fresh_values.reshape(seqs, proposals, kv_heads, v_dim), (0, 2, 1, 3))
    keys_out = jax.vmap(place_rows)(cache_keys, key_rows, starts)
    values_out = jax.vmap(place_rows)(cache_values, value_rows, starts)
    query_maps = jnp.transpose(queries.reshape(seqs, proposals, kv_heads, group, 2, qk_dim), (4, 0, 2, 3, 1, 5))

    def visit(carry, block):
        offset = block * span_len
        block_keys = lax.dynamic_slice_in_dim(keys_out, offset, span_len, 2)
        block_values = lax.dynamic_slice_in_dim(values_out, offset, span_len, 2)
        allowed = block_mask(reach, starts, offset, span_len, proposals)
        members = block_partials(query_maps, block_keys, block_values, allowed)
        return (absorb(carry, tuple((member[None] for member in members)), offset), None)
    stat_shape = (2, seqs, kv_heads, group, proposals)
    initial = (jnp.full(stat_shape, NEG_FILL, jnp.float32), jnp.zeros(stat_shape, jnp.float32), jnp.zeros(stat_shape + (v_dim,), jnp.float32))
    final, unused_out = lax.scan(visit, initial, jnp.arange(N_KV, dtype=jnp.int32))
    attended = final[2] / final[1][..., None]
    lam_heads = mix_lambda.reshape(kv_heads, group)[None, :, :, None, None]
    difference = attended[0] - lam_heads * attended[1]
    head_out = (difference * lax.rsqrt(lax.optimization_barrier(jnp.mean(difference * difference, axis=-1, keepdims=True)) + NORM_EPS) * head_gain.astype(jnp.float32)).astype(jnp.bfloat16)
    head_rows = jnp.transpose(head_out, (0, 3, 1, 2, 4)).reshape(seqs * proposals, heads * v_dim)
    mixed = jnp.dot(head_rows, out_weight, preferred_element_type=jnp.float32).astype(jnp.bfloat16)
    return (mixed.reshape(seqs, proposals, width), keys_out, values_out)
```

```python
import functools

import jax
import jax.numpy as jnp
from jax import lax
from jax.experimental import pallas as pl
from jax.experimental.pallas import tpu as pltpu
from jax.sharding import PartitionSpec as P

NEG_FILL = -1e30
ROTARY_BASE = 10000.0
NORM_EPS = 1e-06
CORES = 2
F32 = jnp.float32
BF16 = jnp.bfloat16
VM = pl.BlockSpec(memory_space=pltpu.VMEM)
SM = pl.BlockSpec(memory_space=pltpu.SMEM)


def sds(shape, dtype):
    return jax.ShapeDtypeStruct(shape, dtype)


def dot_nt(a, b):
    return lax.dot_general(a, b, (((1,), (1,)), ((), ())), preferred_element_type=F32)


def dot_nn(a, b):
    return lax.dot_general(a, b, (((1,), (0,)), ((), ())), preferred_element_type=F32)


def prep_kernel(wq, wk, wv, out, *, kv_heads, group, qk):
    chips = out.shape[0]
    rows = out.shape[1] // kv_heads
    parts = chips // (2 * group)
    quarter = qk // 2 // parts
    key_parts = chips // 4
    key_rows = qk // 2 // key_parts
    width = 2 * qk
    val_rows = width // (chips // 2)
    for g in range(kv_heads):
        base = rows * g
        for r in range(group):
            h = g * group + r
            t = wq[:, width * h : width * (h + 1)].astype(F32).T
            for m in range(2):
                for part in range(parts):
                    z = (r * 2 + m) * parts + part
                    lo = qk * m + quarter * part
                    hi = lo + qk // 2
                    out[z, base : base + quarter] = t[lo : lo + quarter].astype(BF16)
                    out[z, base + quarter : base + 2 * quarter] = t[hi : hi + quarter].astype(BF16)
        tk = wk[:, width * g : width * (g + 1)].astype(F32).T
        tv = wv[:, width * g : width * (g + 1)].astype(F32).T
        off = base + 2 * quarter
        for m in range(2):
            for part in range(key_parts):
                lo = qk * m + key_rows * part
                hi = lo + qk // 2
                both = jnp.concatenate([tk[lo : lo + key_rows], tk[hi : hi + key_rows]], axis=0)
                out[m * key_parts + part, off : off + 2 * key_rows] = both.astype(BF16)
        for y in range(chips // 2):
            out[chips // 2 + y, off : off + val_rows] = tv[
                val_rows * y : val_rows * (y + 1)
            ].astype(BF16)


def norm_kernel(tokens, gain, linked, normed, reach, depth):
    x = tokens[...].astype(F32)
    mean = jnp.mean(x * x, axis=-1, keepdims=True)
    normed[...] = (x * lax.rsqrt(mean + NORM_EPS) * gain[...].astype(F32)).astype(BF16)

    @pl.when(pl.program_id(0) == 0)
    def _():
        r = linked[...]
        for _step in range(5):
            r = jnp.minimum(dot_nn(r, r), 1.0).astype(BF16)
        reach[...] = r
        depth[...] = dot_nt(jnp.ones((8, r.shape[1]), BF16), r) - 1.0


def dot_kernel(sc, x, w, keep, send, scr):
    core = sc[0]
    chips, rows, slab = w.shape
    acc = jnp.zeros((rows, x.shape[0]), F32)
    for z in range(chips):
        at = pl.multiple_of((CORES * z + core) * slab, slab)
        acc = acc + dot_nt(w[z], x[:, pl.ds(at, slab)])
    scr[...] = acc
    half = rows // CORES
    keep[...] = scr[pl.ds(pl.multiple_of(half * core, 8), half)]
    send[...] = scr[pl.ds(pl.multiple_of(half * (1 - core), 8), half)]


def rotate_kernel(sc, keep, recv, cos, sin, out, *, quarter, key_rows):
    p = keep[...] + recv[...]
    chips = out.shape[0]
    chip = sc[1]
    at_q = pl.multiple_of(sc[2] * quarter, 8)
    at_k = pl.multiple_of(sc[3] * key_rows, 8)
    cq, sq = cos[pl.ds(at_q, quarter)], sin[pl.ds(at_q, quarter)]
    is_key = chip < chips // 2
    ck = jnp.where(is_key, cos[pl.ds(at_k, key_rows)], 1.0)
    sk = jnp.where(is_key, sin[pl.ds(at_k, key_rows)], 0.0)
    a, c = p[:quarter], p[quarter : 2 * quarter]
    ka = p[2 * quarter : 2 * quarter + key_rows]
    kc = p[2 * quarter + key_rows :]
    turned = jnp.concatenate(
        [a * cq - c * sq, c * cq + a * sq, ka * ck - kc * sk, kc * ck + ka * sk], axis=0
    ).astype(BF16)
    for z in range(chips):
        out[z] = turned


def attend_kernel(sc, recv, reach, ck, cv, *refs, group, qk, quarter, key_rows, aliased):
    if aliased:
        refs = refs[2:]
    ko, vo, acc_out, stat_out, qs, kf, vf = refs
    chips = recv.shape[0]
    parts = chips // (2 * group)
    key_parts = chips // 4
    step = pl.program_id(0)
    per_step = ck.shape[0]
    span = ck.shape[2]
    width = 2 * qk
    proposals = 16
    n_tok = reach.shape[0]

    @pl.when(step == 0)
    def _():
        for r in range(group):
            pieces = []
            for m in range(2):
                v = (r * 2 + m) * parts
                pieces += [recv[v + p, 0:quarter] for p in range(parts)]
                pieces += [recv[v + p, quarter : 2 * quarter] for p in range(parts)]
            qs[r] = jnp.concatenate(pieces, axis=0).astype(F32).T.astype(BF16)
        lo = 2 * quarter
        pieces = []
        for m in range(2):
            both = [recv[m * key_parts + p, lo:].astype(F32) for p in range(key_parts)]
            pieces += [t[:key_rows] for t in both] + [t[key_rows:] for t in both]
        kf[...] = jnp.concatenate(pieces, axis=0).T.astype(BF16)
        pieces = [recv[chips // 2 + y, lo:] for y in range(chips // 2)]
        vf[...] = jnp.concatenate(pieces, axis=0).astype(F32).T.astype(BF16)

    offset = sc[4]
    lane = lax.broadcasted_iota(jnp.int32, (1, width), 1)
    maps = [(lane < qk).astype(F32).astype(BF16), (lane >= qk).astype(F32).astype(BF16)]
    for k in range(per_step):
        b = step * per_step + k
        start = sc[8 + b]
        row0 = pl.multiple_of(b * proposals, proposals)
        shift = offset - start
        touches = (shift < proposals) & (shift + span > 0)
        ko[k, 0] = ck[k, 0]
        vo[k, 0] = cv[k, 0]

        @pl.when(touches)
        def _():
            rel = lax.broadcasted_iota(jnp.int32, (span, n_tok), 0) + shift
            col = lax.broadcasted_iota(jnp.int32, (span, n_tok), 1) - row0
            inside = (rel >= 0) & (rel < proposals)
            onehot = jnp.where(inside & (rel == col), 1.0, 0.0).astype(BF16)
            written = inside[:, :width]
            ko[k, 0] = jnp.where(written, dot_nn(onehot, kf[...]), ck[k, 0].astype(F32)).astype(BF16)
            vo[k, 0] = jnp.where(written, dot_nn(onehot, vf[...]), cv[k, 0].astype(F32)).astype(BF16)

        rel = lax.broadcasted_iota(jnp.int32, (n_tok, span), 1) + shift
        row = lax.broadcasted_iota(jnp.int32, (n_tok, span), 0) - row0
        hot = jnp.where((rel == row) & (row >= 0) & (row < proposals), 1.0, 0.0).astype(BF16)
        in_tree = dot_nn(reach[pl.ds(row0, proposals), :], hot)
        rel16 = lax.broadcasted_iota(jnp.int32, (proposals, span), 1) + shift
        open16 = jnp.where(rel16 < 0, 1.0, in_tree)
        opened = jnp.concatenate([open16] * (2 * group), axis=0) > 0.5
        rows = []
        for rh in range(2):
            for m in range(2):
                for r2 in range(group // 2):
                    rows.append(qs[rh * (group // 2) + r2, pl.ds(row0, proposals), :] * maps[m])
        q = jnp.concatenate(rows, axis=0)
        s = dot_nt(q, ko[k, 0]) * (qk ** (-0.5))
        top = jnp.max(jnp.where(opened, s, NEG_FILL), axis=1, keepdims=True)
        w = jnp.where(opened, jnp.exp(s - top), 0.0)
        total = jnp.sum(w, axis=1, keepdims=True)
        acc_out[k] = dot_nn(w.astype(BF16), vo[k, 0]).astype(BF16)
        lanes = lax.broadcasted_iota(jnp.int32, (q.shape[0], 128), 1)
        stat = jnp.where(lanes == 0, top, jnp.where(lanes == 1, total, 0.0))
        stat_out[k] = stat.T[:8]


def split3(x):
    hi = x.astype(BF16).astype(F32)
    mid = (x - hi).astype(BF16).astype(F32)
    lo = (x - hi - mid).astype(BF16).astype(F32)
    return [hi, mid, lo]


def pair_kernel(acc0, stat0, acc1, stat1, out):
    seqs, rows, _ = acc0.shape
    half = rows // 2
    for b in range(seqs):
        t0, n0 = stat0[b, 0:1], stat0[b, 1:2]
        t1, n1 = stat1[b, 0:1], stat1[b, 1:2]
        top = jnp.maximum(t0, t1)
        e0, e1 = jnp.exp(t0 - top), jnp.exp(t1 - top)
        total = n0 * e0 + n1 * e1
        cols = jnp.concatenate([e0, e1, jnp.zeros((6, rows), F32)], axis=0).T
        acc = acc0[b].astype(F32) * cols[:, 0:1] + acc1[b].astype(F32) * cols[:, 1:2]
        acc = acc.astype(BF16)
        info = jnp.concatenate(split3(top) + split3(total) + [jnp.zeros((2, rows), F32)], axis=0)
        for rh in range(2):
            out[2 * b + rh, 0:half] = acc[half * rh : half * (rh + 1)]
            view = info if rh == 0 else pltpu.roll(info, half, 1)
            out[2 * b + rh, half : half + 8] = view.astype(BF16)


def finish_kernel(lam, recv, gain, out):
    chips, full, _ = recv.shape
    half = full - 8
    tops, totals = [], []
    for s in range(chips):
        info = recv[s, half:].astype(F32)
        tops.append(info[0:1] + info[1:2] + info[2:3])
        totals.append(info[3:4] + info[4:5] + info[5:6])
    tops = jnp.concatenate(tops, axis=0)
    totals = jnp.concatenate(totals, axis=0)
    scale = jnp.exp(tops - jnp.max(tops, axis=0, keepdims=True))
    den = jnp.sum(scale * totals, axis=0, keepdims=True)
    cols = jnp.concatenate([scale, den, jnp.zeros((7, scale.shape[1]), F32)], axis=0).T[:half]
    num = recv[0, 0:half].astype(F32) * cols[:, 0:1]
    for s in range(1, chips):
        num = num + recv[s, 0:half].astype(F32) * cols[:, s : s + 1]
    attended = num / cols[:, chips : chips + 1]
    quarter = half // 2
    row = lax.broadcasted_iota(jnp.int32, (quarter, 1), 0)
    lam_col = jnp.where(row < quarter // 2, lam[0], lam[1])
    diff = attended[:quarter] - lam_col * attended[quarter:]
    mean = jnp.mean(diff * diff, axis=-1, keepdims=True)
    res = (diff * lax.rsqrt(mean + NORM_EPS) * gain[...].astype(F32)).astype(BF16)
    for z in range(chips):
        out[z] = res


def out_kernel(sc, mine, other, w, out, *, group):
    chips, _, v_dim = mine.shape
    core = sc[0]
    total = jnp.zeros((chips // 2 * 16, w.shape[1]), F32)
    for src, g in ((mine, 1 - core), (other, core)):
        for rh in range(2):
            for r2 in range(group // 2):
                x = jnp.concatenate(
                    [src[2 * b + rh, 16 * r2 : 16 * (r2 + 1)] for b in range(chips // 2)], axis=0
                )
                at = pl.multiple_of((g * group + rh * (group // 2) + r2) * v_dim, v_dim)
                total = total + dot_nn(x, w[pl.ds(at, v_dim)])
    res = total.astype(BF16)
    for t in range(out.shape[0]):
        out[t] = res


def sum_kernel(parts, out):
    total = parts[0].astype(F32)
    for t in range(1, parts.shape[0]):
        total = total + parts[t].astype(F32)
    out[...] = total.astype(BF16)


def on_device(
    tokens,
    norm_gain,
    query_weight,
    key_weight,
    value_weight,
    out_weight,
    head_gain,
    mix_lambda,
    cache_keys,
    cache_values,
    lengths,
    accepted,
    parents,
):
    seqs, proposals, width = tokens.shape
    n_tok = seqs * proposals
    local_kv, span = cache_keys.shape[1:3]
    group = mix_lambda.shape[0] // local_kv
    qk = cache_keys.shape[-1] // 2
    v_dim = cache_values.shape[-1]
    shards = lax.axis_size("kv")
    tps = lax.axis_size("tp")
    chips = shards // CORES
    cols = query_weight.shape[1] + key_weight.shape[1] + value_weight.shape[1]
    rows = cols // shards
    parts = chips // (2 * group)
    quarter = qk // 2 // parts
    key_rows = qk // 2 // (chips // 4)
    me = lax.axis_index("kv")
    chip, core = me // CORES, me % CORES
    same_core = [[CORES * z + c for z in range(chips)] for c in range(CORES)]
    pairs = [(i, i ^ 1) for i in range(shards)]

    def over_chips(x):
        return lax.all_to_all(x, "kv", 0, 0, axis_index_groups=same_core, tiled=True)

    def swap(x):
        return lax.ppermute(x, "kv", pairs)

    weights = pl.pallas_call(
        functools.partial(prep_kernel, kv_heads=local_kv, group=group, qk=qk),
        out_shape=sds((chips, cols // chips, query_weight.shape[0]), BF16),
        in_specs=[VM] * 3,
        out_specs=VM,
        name="prep",
    )(query_weight, key_weight, value_weight)
    weights = over_chips(weights)

    starts = lengths + accepted
    tok = jnp.arange(n_tok, dtype=jnp.int32)
    up = parents.reshape(n_tok) + tok // proposals * proposals
    linked = ((up[:, None] == tok[None, :]) & (tok[:, None] % proposals > 0)) | (
        tok[:, None] == tok[None, :]
    )
    blocks = 4
    normed, reach, depth = pl.pallas_call(
        norm_kernel,
        grid=(blocks,),
        out_shape=(
            sds((n_tok, width), BF16),
            sds((n_tok, n_tok), BF16),
            sds((8, n_tok), F32),
        ),
        in_specs=[
            pl.BlockSpec((n_tok // blocks, width), lambda i: (i, 0)),
            pl.BlockSpec((1, width), lambda i: (0, 0)),
            pl.BlockSpec((n_tok, n_tok), lambda i: (0, 0)),
        ],
        out_specs=(
            pl.BlockSpec((n_tok // blocks, width), lambda i: (i, 0)),
            pl.BlockSpec((n_tok, n_tok), lambda i: (0, 0)),
            pl.BlockSpec((8, n_tok), lambda i: (0, 0)),
        ),
        name="norm",
    )(tokens.reshape(n_tok, width), norm_gain.reshape(1, width), linked.astype(BF16))
    position = jnp.repeat(starts, proposals) + depth[0].astype(jnp.int32)
    inverse = ROTARY_BASE ** (-jnp.arange(qk // 2, dtype=F32) / (qk // 2))
    angles = position.astype(F32)[None, :] * inverse[:, None]
    cosine, sine = jnp.cos(angles), jnp.sin(angles)

    scalars = jnp.concatenate(
        [
            jnp.stack(
                [
                    core,
                    chip,
                    chip % parts,
                    chip % (chips // 4),
                    me * span,
                    1 - core,
                    lax.axis_index("tp"),
                    chip,
                ]
            ).astype(jnp.int32),
            starts,
        ]
    )
    keep, send = pl.pallas_call(
        dot_kernel,
        out_shape=(sds((rows, n_tok), F32), sds((rows, n_tok), F32)),
        in_specs=[SM, VM, VM],
        out_specs=(VM, VM),
        scratch_shapes=[pltpu.VMEM((rows * CORES, n_tok), F32)],
        name="project",
    )(scalars, normed, weights)
    projected = pl.pallas_call(
        functools.partial(rotate_kernel, quarter=quarter, key_rows=key_rows),
        out_shape=sds((chips, rows, n_tok), BF16),
        in_specs=[SM, VM, VM, VM, VM],
        out_specs=VM,
        name="turn",
    )(scalars, keep, swap(send), cosine, sine)
    near = over_chips(projected)
    far = swap(near)

    per_step = 2
    stat_shape = (seqs, 8, 2 * group * proposals)

    def attend(head_slot, recv, held):
        aliased = held is not None

        def cache_map(i, sc):
            return (i, sc[head_slot], 0, 0)

        cache_spec = pl.BlockSpec((per_step, 1, span, v_dim), cache_map)
        whole3 = pl.BlockSpec((chips, rows, n_tok), lambda i, sc: (0, 0, 0))
        whole2 = pl.BlockSpec((n_tok, n_tok), lambda i, sc: (0, 0))
        in_specs = [whole3, whole2, cache_spec, cache_spec]
        operands = [recv, reach, cache_keys, cache_values]
        aliases = {}
        if aliased:
            in_specs += [pl.BlockSpec(memory_space=pl.ANY)] * 2
            operands += list(held)
            aliases = {5: 0, 6: 1}
        return pl.pallas_call(
            functools.partial(
                attend_kernel,
                group=group,
                qk=qk,
                quarter=quarter,
                key_rows=key_rows,
                aliased=aliased,
            ),
            grid_spec=pltpu.PrefetchScalarGridSpec(
                num_scalar_prefetch=1,
                grid=(seqs // per_step,),
                in_specs=in_specs,
                out_specs=(
                    cache_spec,
                    cache_spec,
                    pl.BlockSpec(
                        (per_step, 2 * group * proposals, v_dim), lambda i, sc: (i, 0, 0)
                    ),
                    pl.BlockSpec((per_step,) + stat_shape[1:], lambda i, sc: (i, 0, 0)),
                ),
                scratch_shapes=[
                    pltpu.VMEM((group, n_tok, 2 * qk), BF16),
                    pltpu.VMEM((n_tok, 2 * qk), BF16),
                    pltpu.VMEM((n_tok, v_dim), BF16),
                ],
            ),
            out_shape=(
                sds(cache_keys.shape, BF16),
                sds(cache_values.shape, BF16),
                sds((seqs, 2 * group * proposals, v_dim), BF16),
                sds(stat_shape, F32),
            ),
            input_output_aliases=aliases,
            name="attend_far" if aliased else "attend_near",
        )(scalars, *operands)

    keys_half, values_half, acc_near, stat_near = attend(0, near, None)
    acc_in, stat_in = swap(acc_near), swap(stat_near)
    keys_out, values_out, acc_far, stat_far = attend(5, far, (keys_half, values_half))
    half = group * proposals
    pieces = pl.pallas_call(
        pair_kernel,
        out_shape=sds((chips, half + 8, v_dim), BF16),
        in_specs=[VM] * 4,
        out_specs=VM,
        name="pair",
    )(acc_far, stat_far, acc_in, stat_in)
    pieces = over_chips(pieces)
    first_head = (1 - core) * group + (chip % 2) * (group // 2)
    lam = lax.dynamic_slice_in_dim(mix_lambda, first_head, group // 2, 0)
    heads = pl.pallas_call(
        finish_kernel,
        out_shape=sds((chips, half // 2, v_dim), BF16),
        in_specs=[SM, VM, VM],
        out_specs=VM,
        name="finish",
    )(lam, pieces, head_gain.reshape(1, v_dim))
    heads_near = over_chips(heads)
    heads_far = swap(heads_near)
    local_rows = local_kv * group * v_dim
    out_cols = out_weight.shape[1]
    term = pl.pallas_call(
        functools.partial(out_kernel, group=group),
        grid_spec=pltpu.PrefetchScalarGridSpec(
            num_scalar_prefetch=1,
            grid=(1,),
            in_specs=[
                pl.BlockSpec((chips, half // 2, v_dim), lambda i, sc: (0, 0, 0)),
                pl.BlockSpec((chips, half // 2, v_dim), lambda i, sc: (0, 0, 0)),
                pl.BlockSpec((local_rows, out_cols), lambda i, sc: (sc[6], 0)),
            ],
            out_specs=pl.BlockSpec((tps, n_tok, out_cols), lambda i, sc: (0, 0, 0)),
        ),
        out_shape=sds((tps, n_tok, out_cols), BF16),
        name="project_out",
    )(scalars, heads_near, heads_far, out_weight)
    term = lax.all_to_all(term, "tp", 0, 0, tiled=True)
    mixed = pl.pallas_call(
        sum_kernel,
        out_shape=sds((n_tok, out_cols), BF16),
        in_specs=[VM],
        out_specs=VM,
        name="sum_terms",
    )(term)
    return (mixed.reshape(seqs, proposals, out_cols), keys_out, values_out)


def solution(mesh):
    in_specs = (
        P("grp", None, None),
        P(),
        P("kv", "tp"),
        P("kv", "tp"),
        P("kv", "tp"),
        P(None, "kv"),
        P(),
        P("tp"),
        P("grp", "tp", "kv", None),
        P("grp", "tp", "kv", None),
        P("grp"),
        P("grp"),
        P("grp", None),
    )
    out_specs = (P("grp", None, "kv"), P("grp", "tp", "kv", None), P("grp", "tp", "kv", None))
    return jax.shard_map(
        on_device, mesh=mesh, in_specs=in_specs, out_specs=out_specs, check_vma=False
    )
```

```python
import functools

import jax
import jax.numpy as jnp
from jax import lax
from jax.experimental import pallas as pl
from jax.experimental.pallas import tpu as pltpu
from jax.sharding import PartitionSpec as P

NEG_FILL = -1e30
ROTARY_BASE = 10000.0
NORM_EPS = 1e-06
CORES = 2
F32 = jnp.float32
BF16 = jnp.bfloat16
VM = pl.BlockSpec(memory_space=pltpu.VMEM)
SM = pl.BlockSpec(memory_space=pltpu.SMEM)


def limit(mib):
    return pltpu.CompilerParams(vmem_limit_bytes=mib << 20)


def sds(shape, dtype):
    return jax.ShapeDtypeStruct(shape, dtype)


def dot_nt(a, b):
    return lax.dot_general(a, b, (((1,), (1,)), ((), ())), preferred_element_type=F32)


def dot_nn(a, b):
    return lax.dot_general(a, b, (((1,), (0,)), ((), ())), preferred_element_type=F32)


def prep_kernel(wq_hbm, wk_hbm, wv_hbm, out, wq, wk, wv, sems, *, kv_heads, group, qk):
    copies = [
        pltpu.make_async_copy(src, dst, sems.at[n])
        for n, (src, dst) in enumerate([(wk_hbm, wk), (wv_hbm, wv), (wq_hbm, wq)])
    ]
    for copy in copies:
        copy.start()
    for copy in copies:
        copy.wait()
    chips = out.shape[0]
    rows = out.shape[1] // kv_heads
    parts = chips // (2 * group)
    quarter = qk // 2 // parts
    key_parts = chips // 4
    key_rows = qk // 2 // key_parts
    width = 2 * qk
    val_rows = width // (chips // 2)
    for g in range(kv_heads):
        base = rows * g
        for r in range(group):
            h = g * group + r
            t = wq[:, width * h : width * (h + 1)].astype(F32).T
            for m in range(2):
                for part in range(parts):
                    z = (r * 2 + m) * parts + part
                    lo = qk * m + quarter * part
                    hi = lo + qk // 2
                    out[z, base : base + quarter] = t[lo : lo + quarter].astype(BF16)
                    out[z, base + quarter : base + 2 * quarter] = t[hi : hi + quarter].astype(BF16)
        tk = wk[:, width * g : width * (g + 1)].astype(F32).T
        tv = wv[:, width * g : width * (g + 1)].astype(F32).T
        off = base + 2 * quarter
        for m in range(2):
            for part in range(key_parts):
                lo = qk * m + key_rows * part
                hi = lo + qk // 2
                both = jnp.concatenate([tk[lo : lo + key_rows], tk[hi : hi + key_rows]], axis=0)
                out[m * key_parts + part, off : off + 2 * key_rows] = both.astype(BF16)
        for y in range(chips // 2):
            out[chips // 2 + y, off : off + val_rows] = tv[
                val_rows * y : val_rows * (y + 1)
            ].astype(BF16)


def norm_kernel(tokens, gain, linked, normed, reach, depth):
    x = tokens[...].astype(F32)
    mean = jnp.mean(x * x, axis=-1, keepdims=True)
    normed[...] = (x * lax.rsqrt(mean + NORM_EPS) * gain[...].astype(F32)).astype(BF16)

    @pl.when(pl.program_id(0) == 0)
    def _():
        r = linked[...]
        for _step in range(5):
            r = jnp.minimum(dot_nn(r, r), 1.0).astype(BF16)
        reach[...] = r
        depth[...] = dot_nt(jnp.ones((8, r.shape[1]), BF16), r) - 1.0


def place():
    me = lax.axis_index("kv")
    return me, lax.div(me, CORES), lax.rem(me, CORES)


def dot_kernel(x, w, keep, send, scr):
    _, _, core = place()
    chips, rows, slab = w.shape
    acc = jnp.zeros((rows, x.shape[0]), F32)
    for z in range(chips):
        at = pl.multiple_of((CORES * z + core) * slab, slab)
        acc = acc + dot_nt(w[z], x[:, pl.ds(at, slab)])
    scr[...] = acc
    half = rows // CORES
    keep[...] = scr[pl.ds(pl.multiple_of(half * core, 8), half)]
    send[...] = scr[pl.ds(pl.multiple_of(half * (1 - core), 8), half)]


def rotate_kernel(keep, recv, table, out, *, quarter, key_rows):
    p = keep[...] + recv[...]
    chips = out.shape[0]
    _, chip, _ = place()
    freqs = table.shape[0] // 2
    at_q = pl.multiple_of(lax.rem(chip, freqs // quarter) * quarter, 8)
    at_k = pl.multiple_of(lax.rem(chip, freqs // key_rows) * key_rows, 8)
    cq, sq = table[pl.ds(at_q, quarter)], table[pl.ds(at_q + freqs, quarter)]
    cos_k, sin_k = table[pl.ds(at_k, key_rows)], table[pl.ds(at_k + freqs, key_rows)]
    is_key = chip < chips // 2
    ck = jnp.where(is_key, cos_k, 1.0)
    sk = jnp.where(is_key, sin_k, 0.0)
    a, c = p[:quarter], p[quarter : 2 * quarter]
    ka = p[2 * quarter : 2 * quarter + key_rows]
    kc = p[2 * quarter + key_rows :]
    turned = jnp.concatenate(
        [a * cq - c * sq, c * cq + a * sq, ka * ck - kc * sk, kc * ck + ka * sk], axis=0
    ).astype(BF16)
    for z in range(chips):
        out[z] = turned


def attend_kernel(
    lengths, accepted, recv, reach, ck, cv, acc_out, stat_out, kf, vf, qs, *, qk, quarter, key_rows, side
):
    chips = recv.shape[0]
    group = qs.shape[0]
    parts = chips // (2 * group)
    key_parts = chips // 4
    seqs, _, span, width = ck.shape
    n_tok = reach.shape[0]
    proposals = n_tok // seqs
    me, _, core = place()
    g = core if side == 0 else 1 - core
    scale = qk ** (-0.5)
    for r in range(group):
        pieces = []
        for m in range(2):
            v = (r * 2 + m) * parts
            pieces += [recv[v + p, 0:quarter] for p in range(parts)]
            pieces += [recv[v + p, quarter : 2 * quarter] for p in range(parts)]
        qs[r] = (jnp.concatenate(pieces, axis=0).astype(F32).T * scale).astype(BF16)
    lo = 2 * quarter
    pieces = []
    for m in range(2):
        both = [recv[m * key_parts + p, lo:].astype(F32) for p in range(key_parts)]
        pieces += [t[:key_rows] for t in both] + [t[key_rows:] for t in both]
    kf[...] = jnp.concatenate(pieces, axis=0).T.astype(BF16)
    pieces = [recv[chips // 2 + y, lo:] for y in range(chips // 2)]
    vf[...] = jnp.concatenate(pieces, axis=0).astype(F32).T.astype(BF16)

    lane = lax.broadcasted_iota(jnp.int32, (1, width), 1)
    maps = [(lane < qk).astype(F32).astype(BF16), (lane >= qk).astype(F32).astype(BF16)]
    n_rows = 2 * group * proposals
    slot = lax.rem(lax.broadcasted_iota(jnp.int32, (proposals, n_tok), 1), proposals)
    cached = lax.broadcasted_iota(jnp.int32, (1, span), 1)
    for b in range(seqs):
        row0 = b * proposals
        shift = me * span - lengths[b] - accepted[b]
        rows = []
        for rh in range(2):
            for m in range(2):
                for r2 in range(group // 2):
                    rows.append(qs[rh * (group // 2) + r2, row0 : row0 + proposals] * maps[m])
        q = jnp.concatenate(rows, axis=0)
        old = dot_nt(q, ck[b, g]) + jnp.where(cached + shift < 0, 0.0, NEG_FILL)
        at = slot - shift
        seen = (reach[row0 : row0 + proposals].astype(F32) > 0.5) & (at >= 0) & (at < span)
        new = dot_nt(q, kf[...]).reshape(2 * group, proposals, n_tok)
        new = (new + jnp.where(seen, 0.0, NEG_FILL)[None]).reshape(n_rows, n_tok)
        top = jnp.maximum(
            jnp.max(old, axis=1, keepdims=True), jnp.max(new, axis=1, keepdims=True)
        )
        base = jnp.maximum(top, 0.5 * NEG_FILL)
        w_old, w_new = jnp.exp(old - base), jnp.exp(new - base)
        total = jnp.sum(w_old, axis=1, keepdims=True) + jnp.sum(w_new, axis=1, keepdims=True)
        acc = dot_nn(w_old.astype(BF16), cv[b, g]) + dot_nn(w_new.astype(BF16), vf[...])
        acc_out[b] = acc.astype(BF16)
        lanes = lax.broadcasted_iota(jnp.int32, (n_rows, 128), 1)
        stat = jnp.where(lanes == 0, top, jnp.where(lanes == 1, total, 0.0))
        stat_out[b] = stat.T[:8]


def store_kernel(lengths, accepted, ck, cv, kn, vn, kfar, vfar, ko, vo):
    me, _, core = place()
    b = pl.program_id(0)
    heads, span, width = ck.shape[1:]
    n_tok = kn.shape[0]
    proposals = n_tok // pl.num_programs(0)
    shift = me * span - lengths[b] - accepted[b]
    ko[...] = ck[...]
    vo[...] = cv[...]

    @pl.when((shift < proposals) & (shift + span > 0))
    def _():
        rel = lax.broadcasted_iota(jnp.int32, (span, n_tok), 0) + shift
        col = lax.broadcasted_iota(jnp.int32, (span, n_tok), 1) - b * proposals
        inside = (rel >= 0) & (rel < proposals)
        onehot = jnp.where(inside & (rel == col), 1.0, 0.0).astype(BF16)
        rel = lax.broadcasted_iota(jnp.int32, (span, width), 0) + shift
        written = (rel >= 0) & (rel < proposals)
        for g in range(heads):
            near = jnp.where(core == g, 1.0, 0.0)
            for fresh_n, fresh_f, old, new in ((kn, kfar, ck, ko), (vn, vfar, cv, vo)):
                fresh = fresh_n[...].astype(F32) * near + fresh_f[...].astype(F32) * (1.0 - near)
                placed = dot_nn(onehot, fresh.astype(BF16))
                new[0, g] = jnp.where(written, placed, old[0, g].astype(F32)).astype(BF16)


def split3(x):
    hi = x.astype(BF16).astype(F32)
    mid = (x - hi).astype(BF16).astype(F32)
    lo = (x - hi - mid).astype(BF16).astype(F32)
    return [hi, mid, lo]


def pair_kernel(acc0, stat0, acc1, stat1, out):
    seqs, rows, _ = acc0.shape
    half = rows // 2
    for b in range(seqs):
        t0, n0 = stat0[b, 0:1], stat0[b, 1:2]
        t1, n1 = stat1[b, 0:1], stat1[b, 1:2]
        top = jnp.maximum(t0, t1)
        e0, e1 = jnp.exp(t0 - top), jnp.exp(t1 - top)
        total = n0 * e0 + n1 * e1
        cols = jnp.concatenate([e0, e1, jnp.zeros((6, rows), F32)], axis=0).T
        acc = acc0[b].astype(F32) * cols[:, 0:1] + acc1[b].astype(F32) * cols[:, 1:2]
        acc = acc.astype(BF16)
        info = jnp.concatenate(split3(top) + split3(total) + [jnp.zeros((2, rows), F32)], axis=0)
        for rh in range(2):
            out[2 * b + rh, 0:half] = acc[half * rh : half * (rh + 1)]
            view = info if rh == 0 else pltpu.roll(info, half, 1)
            out[2 * b + rh, half : half + 8] = view.astype(BF16)


def finish_kernel(lam, recv, gain, out):
    chips, full, _ = recv.shape
    half = full - 8
    tops, totals = [], []
    for s in range(chips):
        info = recv[s, half:].astype(F32)
        tops.append(info[0:1] + info[1:2] + info[2:3])
        totals.append(info[3:4] + info[4:5] + info[5:6])
    tops = jnp.concatenate(tops, axis=0)
    totals = jnp.concatenate(totals, axis=0)
    scale = jnp.exp(tops - jnp.max(tops, axis=0, keepdims=True))
    den = jnp.sum(scale * totals, axis=0, keepdims=True)
    cols = jnp.concatenate([scale, den, jnp.zeros((7, scale.shape[1]), F32)], axis=0).T[:half]
    num = recv[0, 0:half].astype(F32) * cols[:, 0:1]
    for s in range(1, chips):
        num = num + recv[s, 0:half].astype(F32) * cols[:, s : s + 1]
    attended = num / cols[:, chips : chips + 1]
    quarter = half // 2
    row = lax.broadcasted_iota(jnp.int32, (quarter, 1), 0)
    lam_col = jnp.where(row < quarter // 2, lam[0], lam[1])
    diff = attended[:quarter] - lam_col * attended[quarter:]
    mean = jnp.mean(diff * diff, axis=-1, keepdims=True)
    res = (diff * lax.rsqrt(mean + NORM_EPS) * gain[...].astype(F32)).astype(BF16)
    for z in range(chips):
        out[z] = res


def out_kernel(src, held, w, out, *, group, side):
    chips, _, v_dim = src.shape
    total = held[...] if held is not None else None
    _, _, core = place()
    g = 1 - core if side == 0 else core
    for rh in range(2):
        for r2 in range(group // 2):
            x = jnp.concatenate(
                [src[2 * b + rh, 16 * r2 : 16 * (r2 + 1)] for b in range(chips // 2)], axis=0
            )
            at = pl.multiple_of((g * group + rh * (group // 2) + r2) * v_dim, v_dim)
            part = dot_nn(x, w[pl.ds(at, v_dim)])
            total = part if total is None else total + part
    out[...] = total.astype(out.dtype)


def out_near_kernel(tp, src, w, out, *, group):
    out_kernel(src, None, w, out, group=group, side=0)


def out_far_kernel(tp, src, held, w, out, *, group):
    out_kernel(src, held, w, out, group=group, side=1)


def add_kernel(a, b, out):
    out[...] = (a[...].astype(F32) + b[...].astype(F32)).astype(BF16)


def on_device(
    tokens,
    norm_gain,
    query_weight,
    key_weight,
    value_weight,
    out_weight,
    head_gain,
    mix_lambda,
    cache_keys,
    cache_values,
    lengths,
    accepted,
    parents,
):
    seqs, proposals, width = tokens.shape
    n_tok = seqs * proposals
    local_kv, span = cache_keys.shape[1:3]
    group = mix_lambda.shape[0] // local_kv
    qk = cache_keys.shape[-1] // 2
    v_dim = cache_values.shape[-1]
    shards = lax.axis_size("kv")
    tps = lax.axis_size("tp")
    chips = shards // CORES
    cols = query_weight.shape[1] + key_weight.shape[1] + value_weight.shape[1]
    rows = cols // shards
    parts = chips // (2 * group)
    quarter = qk // 2 // parts
    key_rows = qk // 2 // (chips // 4)
    me = lax.axis_index("kv")
    chip, core = me // CORES, me % CORES
    same_core = [[CORES * z + c for z in range(chips)] for c in range(CORES)]
    pairs = [(i, i ^ 1) for i in range(shards)]

    def over_chips(x):
        return lax.all_to_all(x, "kv", 0, 0, axis_index_groups=same_core, tiled=True)

    def swap(x):
        return lax.ppermute(x, "kv", pairs)

    weights = pl.pallas_call(
        functools.partial(prep_kernel, kv_heads=local_kv, group=group, qk=qk),
        out_shape=sds((chips, cols // chips, query_weight.shape[0]), BF16),
        in_specs=[pl.BlockSpec(memory_space=pltpu.HBM)] * 3,
        out_specs=VM,
        scratch_shapes=[
            pltpu.VMEM(query_weight.shape, BF16),
            pltpu.VMEM(key_weight.shape, BF16),
            pltpu.VMEM(value_weight.shape, BF16),
            pltpu.SemaphoreType.DMA((3,)),
        ],
        compiler_params=limit(60),
        name="prep",
    )(query_weight, key_weight, value_weight)
    weights = over_chips(weights)

    starts = lengths + accepted
    tok = jnp.arange(n_tok, dtype=jnp.int32)
    up = parents.reshape(n_tok) + tok // proposals * proposals
    linked = ((up[:, None] == tok[None, :]) & (tok[:, None] % proposals > 0)) | (
        tok[:, None] == tok[None, :]
    )
    blocks = 4
    normed, reach, depth = pl.pallas_call(
        norm_kernel,
        grid=(blocks,),
        out_shape=(
            sds((n_tok, width), BF16),
            sds((n_tok, n_tok), BF16),
            sds((8, n_tok), F32),
        ),
        in_specs=[
            pl.BlockSpec((n_tok // blocks, width), lambda i: (i, 0)),
            pl.BlockSpec((1, width), lambda i: (0, 0)),
            pl.BlockSpec((n_tok, n_tok), lambda i: (0, 0)),
        ],
        out_specs=(
            pl.BlockSpec((n_tok // blocks, width), lambda i: (i, 0)),
            pl.BlockSpec((n_tok, n_tok), lambda i: (0, 0)),
            pl.BlockSpec((8, n_tok), lambda i: (0, 0)),
        ),
        compiler_params=limit(16),
        name="norm",
    )(tokens.reshape(n_tok, width), norm_gain.reshape(1, width), linked.astype(BF16))
    position = jnp.repeat(starts, proposals) + depth[0].astype(jnp.int32)
    inverse = ROTARY_BASE ** (-jnp.arange(qk // 2, dtype=F32) / (qk // 2))
    angles = position.astype(F32)[None, :] * inverse[:, None]
    table = jnp.concatenate([jnp.cos(angles), jnp.sin(angles)], axis=0)
    weights, table = lax.optimization_barrier((weights, table))

    keep, send = pl.pallas_call(
        dot_kernel,
        out_shape=(sds((rows, n_tok), F32), sds((rows, n_tok), F32)),
        in_specs=[VM, VM],
        out_specs=(VM, VM),
        scratch_shapes=[pltpu.VMEM((rows * CORES, n_tok), F32)],
        compiler_params=limit(8),
        name="project",
    )(normed, weights)
    projected = pl.pallas_call(
        functools.partial(rotate_kernel, quarter=quarter, key_rows=key_rows),
        out_shape=sds((chips, rows, n_tok), BF16),
        in_specs=[VM, VM, VM],
        out_specs=VM,
        compiler_params=limit(4),
        name="turn",
    )(keep, swap(send), table)
    near = over_chips(projected)
    far = swap(near)

    n_rows = 2 * group * proposals

    def attend(side, recv):
        return pl.pallas_call(
            functools.partial(
                attend_kernel, qk=qk, quarter=quarter, key_rows=key_rows, side=side
            ),
            in_specs=[SM, SM] + [VM] * 4,
            out_specs=(VM,) * 4,
            out_shape=(
                sds((seqs, n_rows, v_dim), BF16),
                sds((seqs, 8, n_rows), F32),
                sds((n_tok, 2 * qk), BF16),
                sds((n_tok, v_dim), BF16),
            ),
            scratch_shapes=[pltpu.VMEM((group, n_tok, 2 * qk), BF16)],
            compiler_params=limit(16),
            cost_estimate=pl.CostEstimate(
                flops=4 * seqs * n_rows * span * v_dim,
                bytes_accessed=2 * seqs * span * v_dim * 2,
                transcendentals=seqs * n_rows * span,
            ),
            name="attend_far" if side else "attend_near",
        )(lengths, accepted, recv, reach, cache_keys, cache_values)

    acc_near, stat_near, kn, vn = attend(0, near)
    acc_in, stat_in = swap(acc_near), swap(stat_near)
    acc_far, stat_far, kfar, vfar = attend(1, far)
    half = group * proposals
    pieces = pl.pallas_call(
        pair_kernel,
        out_shape=sds((chips, half + 8, v_dim), BF16),
        in_specs=[VM] * 4,
        out_specs=VM,
        compiler_params=limit(8),
        name="pair",
    )(acc_far, stat_far, acc_in, stat_in)
    pieces = over_chips(pieces)
    cache_spec = pl.BlockSpec((1, local_kv, span, v_dim), lambda i: (i, 0, 0, 0))
    fresh_spec = pl.BlockSpec((n_tok, v_dim), lambda i: (0, 0))
    keys_out, values_out = pl.pallas_call(
        store_kernel,
        grid=(seqs,),
        in_specs=[SM, SM, cache_spec, cache_spec] + [fresh_spec] * 4,
        out_specs=(cache_spec, cache_spec),
        out_shape=(sds(cache_keys.shape, BF16), sds(cache_values.shape, BF16)),
        compiler_params=limit(16),
        cost_estimate=pl.CostEstimate(
            flops=4 * seqs * n_rows * span * v_dim,
            bytes_accessed=8 * seqs * local_kv * span * v_dim,
            transcendentals=0,
        ),
        name="store",
    )(lengths, accepted, cache_keys, cache_values, kn, vn, kfar, vfar)
    pieces, keys_out, values_out = lax.optimization_barrier((pieces, keys_out, values_out))
    first_head = (1 - core) * group + (chip % 2) * (group // 2)
    lam = lax.dynamic_slice_in_dim(mix_lambda, first_head, group // 2, 0)
    heads = pl.pallas_call(
        finish_kernel,
        out_shape=sds((chips, half // 2, v_dim), BF16),
        in_specs=[SM, VM, VM],
        out_specs=VM,
        compiler_params=limit(4),
        name="finish",
    )(lam, pieces, head_gain.reshape(1, v_dim))
    heads_near = over_chips(heads)
    heads_far = swap(heads_near)
    local_rows = local_kv * group * v_dim
    out_cols = out_weight.shape[1]
    heads_spec = pl.BlockSpec((chips, half // 2, v_dim), lambda i, tp: (0, 0, 0))
    weight_spec = pl.BlockSpec((local_rows, out_cols), lambda i, tp: (tp[0], 0))
    term_spec = pl.BlockSpec((n_tok, out_cols), lambda i, tp: (0, 0))

    def project_out(body, in_specs, dtype, name, *operands):
        return pl.pallas_call(
            functools.partial(body, group=group),
            grid_spec=pltpu.PrefetchScalarGridSpec(
                num_scalar_prefetch=1, grid=(1,), in_specs=in_specs, out_specs=term_spec
            ),
            out_shape=sds((n_tok, out_cols), dtype),
            compiler_params=limit(4),
            name=name,
        )(lax.axis_index("tp").reshape(1), *operands)

    partial_term = project_out(
        out_near_kernel, [heads_spec, weight_spec], F32, "out_near", heads_near, out_weight
    )
    term = project_out(
        out_far_kernel,
        [heads_spec, term_spec, weight_spec],
        BF16,
        "out_far",
        heads_far,
        partial_term,
        out_weight,
    )

    def add_from(x, hops, name):
        return pl.pallas_call(
            add_kernel,
            out_shape=sds(x.shape, BF16),
            in_specs=[VM] * 2,
            out_specs=VM,
            compiler_params=limit(4),
            name=name,
        )(x, lax.ppermute(x, "tp", hops))

    distance = 1
    while distance < tps:
        pairing = [(t, t // (2 * distance) * 2 * distance + 2 * distance - 1 - t % (2 * distance)) for t in range(tps)]
        term = add_from(term, pairing, "sum_terms")
        distance *= 2
    mixed = term
    return (mixed.reshape(seqs, proposals, out_cols), keys_out, values_out)


def solution(mesh):
    in_specs = (
        P("grp", None, None),
        P(),
        P("kv", "tp"),
        P("kv", "tp"),
        P("kv", "tp"),
        P(None, "kv"),
        P(),
        P("tp"),
        P("grp", "tp", "kv", None),
        P("grp", "tp", "kv", None),
        P("grp"),
        P("grp"),
        P("grp", None),
    )
    out_specs = (P("grp", None, "kv"), P("grp", "tp", "kv", None), P("grp", "tp", "kv", None))
    return jax.shard_map(
        on_device, mesh=mesh, in_specs=in_specs, out_specs=out_specs, check_vma=False
    )
```

```python
import functools

import jax
import jax.numpy as jnp
from jax import lax
from jax.experimental import pallas as pl
from jax.experimental.pallas import tpu as pltpu
from jax.sharding import PartitionSpec as P


NEG_FILL = -1e30
ROTARY_BASE = 10000.0
NORM_EPS = 1e-06
CORES = 2
F32 = jnp.float32
BF16 = jnp.bfloat16
VM = pl.BlockSpec(memory_space=pltpu.VMEM)
SM = pl.BlockSpec(memory_space=pltpu.SMEM)


def limit(mib):
    return pltpu.CompilerParams(vmem_limit_bytes=mib << 20)


def sds(shape, dtype):
    return jax.ShapeDtypeStruct(shape, dtype)


def dot_nt(a, b):
    return lax.dot_general(a, b, (((1,), (1,)), ((), ())), preferred_element_type=F32)


def dot_nn(a, b):
    return lax.dot_general(a, b, (((1,), (0,)), ((), ())), preferred_element_type=F32)


def prep_kernel(wq_hbm, wk_hbm, wv_hbm, out, wq, wk, wv, sems, *, kv_heads, group, qk):
    copies = [
        pltpu.make_async_copy(src, dst, sems.at[n])
        for n, (src, dst) in enumerate([(wk_hbm, wk), (wv_hbm, wv), (wq_hbm, wq)])
    ]
    for copy in copies:
        copy.start()
    for copy in copies:
        copy.wait()
    chips = out.shape[0]
    rows = out.shape[1] // kv_heads
    parts = chips // (2 * group)
    quarter = qk // 2 // parts
    key_parts = chips // 4
    key_rows = qk // 2 // key_parts
    width = 2 * qk
    val_rows = width // (chips // 2)
    for g in range(kv_heads):
        base = rows * g
        for r in range(group):
            h = g * group + r
            t = wq[:, width * h : width * (h + 1)].astype(F32).T
            for m in range(2):
                for part in range(parts):
                    z = (r * 2 + m) * parts + part
                    lo = qk * m + quarter * part
                    hi = lo + qk // 2
                    out[z, base : base + quarter] = t[lo : lo + quarter].astype(BF16)
                    out[z, base + quarter : base + 2 * quarter] = t[hi : hi + quarter].astype(BF16)
        tk = wk[:, width * g : width * (g + 1)].astype(F32).T
        tv = wv[:, width * g : width * (g + 1)].astype(F32).T
        off = base + 2 * quarter
        for m in range(2):
            for part in range(key_parts):
                lo = qk * m + key_rows * part
                hi = lo + qk // 2
                both = jnp.concatenate([tk[lo : lo + key_rows], tk[hi : hi + key_rows]], axis=0)
                out[m * key_parts + part, off : off + 2 * key_rows] = both.astype(BF16)
        for y in range(chips // 2):
            out[chips // 2 + y, off : off + val_rows] = tv[
                val_rows * y : val_rows * (y + 1)
            ].astype(BF16)


def norm_kernel(tokens, gain, linked, normed, reach, depth):
    x = tokens[...].astype(F32)
    mean = jnp.mean(x * x, axis=-1, keepdims=True)
    normed[...] = (x * lax.rsqrt(mean + NORM_EPS) * gain[...].astype(F32)).astype(BF16)

    @pl.when(pl.program_id(0) == 0)
    def _():
        r = linked[...]
        for _ in range(5):
            r = jnp.minimum(dot_nn(r, r), 1.0).astype(BF16)
        reach[...] = r
        depth[...] = dot_nt(jnp.ones((8, r.shape[1]), BF16), r) - 1.0


def place():
    me = lax.axis_index("kv")
    return me, lax.div(me, CORES), lax.rem(me, CORES)


def dot_kernel(x, w, keep, send, scr):
    block, all_rows, slab = w.shape
    _, chip, core = place()
    first = lax.div(chip, block) * block
    acc = jnp.zeros((all_rows, x.shape[0]), F32)
    for i in range(block):
        at = pl.multiple_of((CORES * (first + i) + core) * slab, slab)
        acc = acc + dot_nt(w[i], x[:, pl.ds(at, slab)])
    scr[...] = acc
    rows = all_rows // block // CORES
    for k in range(block):
        base = CORES * rows * k
        keep[rows * k : rows * (k + 1)] = scr[pl.ds(pl.multiple_of(base + rows * core, 8), rows)]
        send[rows * k : rows * (k + 1)] = scr[
            pl.ds(pl.multiple_of(base + rows * (1 - core), 8), rows)
        ]


def gather_kernel(keep, recv, out):
    p = keep[...] + recv[...]
    for t in range(out.shape[0]):
        out[t] = p


def rotate_kernel(parts, table, out, *, quarter, key_rows):
    total = parts[0]
    for t in range(1, parts.shape[0]):
        total = total + parts[t]
    block = out.shape[0]
    _, chip, _ = place()
    freqs = table.shape[0] // 2
    is_key = lax.rem(chip, block) < parts.shape[0] // 2
    rows = total.shape[0] // block
    for k in range(block):
        p = total[rows * k : rows * (k + 1)]
        at_q = k % (freqs // quarter) * quarter
        at_k = k % (freqs // key_rows) * key_rows
        cq, sq = table[at_q : at_q + quarter], table[freqs + at_q : freqs + at_q + quarter]
        ck = jnp.where(is_key, table[at_k : at_k + key_rows], 1.0)
        sk = jnp.where(is_key, table[freqs + at_k : freqs + at_k + key_rows], 0.0)
        a, c = p[:quarter], p[quarter : 2 * quarter]
        ka = p[2 * quarter : 2 * quarter + key_rows]
        kc = p[2 * quarter + key_rows :]
        turned = jnp.concatenate(
            [a * cq - c * sq, c * cq + a * sq, ka * ck - kc * sk, kc * ck + ka * sk], axis=0
        ).astype(BF16)
        for t in range(block):
            out[t, rows * k : rows * (k + 1)] = turned


def attend_kernel(
    lengths, accepted, recv, reach, ck, cv, acc_out, stat_out, fresh, qs, *, qk, quarter, key_rows, side
):
    kf, vf = fresh.at[0], fresh.at[1]
    chips = recv.shape[0]
    group = qs.shape[0]
    parts = chips // (2 * group)
    key_parts = chips // 4
    seqs, _, span, width = ck.shape
    n_tok = reach.shape[0]
    proposals = n_tok // seqs
    me, _, core = place()
    g = core if side == 0 else 1 - core
    scale = qk ** (-0.5)
    for r in range(group):
        pieces = []
        for m in range(2):
            v = (r * 2 + m) * parts
            pieces += [recv[v + p, 0:quarter] for p in range(parts)]
            pieces += [recv[v + p, quarter : 2 * quarter] for p in range(parts)]
        qs[r] = (jnp.concatenate(pieces, axis=0).astype(F32).T * scale).astype(BF16)
    lo = 2 * quarter
    pieces = []
    for m in range(2):
        both = [recv[m * key_parts + p, lo:].astype(F32) for p in range(key_parts)]
        pieces += [t[:key_rows] for t in both] + [t[key_rows:] for t in both]
    kf[...] = jnp.concatenate(pieces, axis=0).T.astype(BF16)
    pieces = [recv[chips // 2 + y, lo:] for y in range(chips // 2)]
    vf[...] = jnp.concatenate(pieces, axis=0).astype(F32).T.astype(BF16)

    lane = lax.broadcasted_iota(jnp.int32, (1, width), 1)
    maps = [(lane < qk).astype(F32).astype(BF16), (lane >= qk).astype(F32).astype(BF16)]
    n_rows = 2 * group * proposals
    slot = lax.rem(lax.broadcasted_iota(jnp.int32, (proposals, n_tok), 1), proposals)
    cached = lax.broadcasted_iota(jnp.int32, (1, span), 1)
    for b in range(seqs):
        row0 = b * proposals
        shift = me * span - lengths[b] - accepted[b]
        rows = []
        for rh in range(2):
            for m in range(2):
                for r2 in range(group // 2):
                    rows.append(qs[rh * (group // 2) + r2, row0 : row0 + proposals] * maps[m])
        q = jnp.concatenate(rows, axis=0)
        old = dot_nt(q, ck[b, g]) + jnp.where(cached + shift < 0, 0.0, NEG_FILL)
        at = slot - shift
        seen = (reach[row0 : row0 + proposals].astype(F32) > 0.5) & (at >= 0) & (at < span)
        new = dot_nt(q, kf[...]).reshape(2 * group, proposals, n_tok)
        new = (new + jnp.where(seen, 0.0, NEG_FILL)[None]).reshape(n_rows, n_tok)
        scores = jnp.concatenate([old, new], axis=1)
        top = jnp.max(scores, axis=1, keepdims=True)
        w = jnp.exp(scores - jnp.maximum(top, 0.5 * NEG_FILL))
        total = jnp.sum(w, axis=1, keepdims=True)
        w = w.astype(BF16)
        acc = dot_nn(w[:, :span], cv[b, g]) + dot_nn(w[:, span:], vf[...])
        acc_out[b] = acc.astype(BF16)
        lanes = lax.broadcasted_iota(jnp.int32, (n_rows, 128), 1)
        stat = jnp.where(lanes == 0, top, jnp.where(lanes == 1, total, 0.0))
        stat_out[b] = stat.T[:8]


def store_kernel(lengths, accepted, ck, cv, fresh_near, fresh_far, ko, vo):
    me, _, core = place()
    b = pl.program_id(0)
    heads, span, width = ck.shape[1:]
    n_tok = fresh_near.shape[1]
    proposals = n_tok // pl.num_programs(0)
    shift = me * span - lengths[b] - accepted[b]
    ko[...] = ck[...]
    vo[...] = cv[...]

    @pl.when((shift < proposals) & (shift + span > 0))
    def _():
        rel = lax.broadcasted_iota(jnp.int32, (span, n_tok), 0) + shift
        col = lax.broadcasted_iota(jnp.int32, (span, n_tok), 1) - b * proposals
        inside = (rel >= 0) & (rel < proposals)
        onehot = jnp.where(inside & (rel == col), 1.0, 0.0).astype(BF16)
        rel = lax.broadcasted_iota(jnp.int32, (span, width), 0) + shift
        written = (rel >= 0) & (rel < proposals)
        for g in range(heads):
            near = jnp.where(core == g, 1.0, 0.0)
            for n, (old, new) in enumerate(((ck, ko), (cv, vo))):
                fresh = fresh_near[n].astype(F32) * near + fresh_far[n].astype(F32) * (1.0 - near)
                placed = dot_nn(onehot, fresh.astype(BF16))
                new[0, g] = jnp.where(written, placed, old[0, g].astype(F32)).astype(BF16)


def split3(x):
    hi = x.astype(BF16).astype(F32)
    mid = (x - hi).astype(BF16).astype(F32)
    lo = (x - hi - mid).astype(BF16).astype(F32)
    return [hi, mid, lo]


def pair_kernel(acc0, stat0, acc1, stat1, out):
    seqs, rows, _ = acc0.shape
    half = rows // 2
    for b in range(seqs):
        t0, n0 = stat0[b, 0:1], stat0[b, 1:2]
        t1, n1 = stat1[b, 0:1], stat1[b, 1:2]
        top = jnp.maximum(t0, t1)
        e0, e1 = jnp.exp(t0 - top), jnp.exp(t1 - top)
        total = n0 * e0 + n1 * e1
        cols = jnp.concatenate([e0, e1, jnp.zeros((6, rows), F32)], axis=0).T
        acc = acc0[b].astype(F32) * cols[:, 0:1] + acc1[b].astype(F32) * cols[:, 1:2]
        acc = acc.astype(BF16)
        info = jnp.concatenate(split3(top) + split3(total) + [jnp.zeros((2, rows), F32)], axis=0)
        for rh in range(2):
            out[2 * b + rh, 0:half] = acc[half * rh : half * (rh + 1)]
            view = info if rh == 0 else pltpu.roll(info, half, 1)
            out[2 * b + rh, half : half + 8] = view.astype(BF16)


def finish_kernel(lam, recv, gain, out):
    chips, full, _ = recv.shape
    half = full - 8
    tops, totals = [], []
    for s in range(chips):
        info = recv[s, half:].astype(F32)
        tops.append(info[0:1] + info[1:2] + info[2:3])
        totals.append(info[3:4] + info[4:5] + info[5:6])
    tops = jnp.concatenate(tops, axis=0)
    totals = jnp.concatenate(totals, axis=0)
    scale = jnp.exp(tops - jnp.max(tops, axis=0, keepdims=True))
    den = jnp.sum(scale * totals, axis=0, keepdims=True)
    cols = jnp.concatenate([scale, den, jnp.zeros((7, scale.shape[1]), F32)], axis=0).T[:half]
    num = recv[0, 0:half].astype(F32) * cols[:, 0:1]
    for s in range(1, chips):
        num = num + recv[s, 0:half].astype(F32) * cols[:, s : s + 1]
    attended = num / cols[:, chips : chips + 1]
    quarter = half // 2
    row = lax.broadcasted_iota(jnp.int32, (quarter, 1), 0)
    lam_col = jnp.where(row < quarter // 2, lam[0], lam[1])
    diff = attended[:quarter] - lam_col * attended[quarter:]
    mean = jnp.mean(diff * diff, axis=-1, keepdims=True)
    res = (diff * lax.rsqrt(mean + NORM_EPS) * gain[...].astype(F32)).astype(BF16)
    for z in range(chips):
        out[z] = res


def out_kernel(src, held, w, out, *, group, side):
    chips, _, v_dim = src.shape
    total = held[...] if held is not None else None
    _, _, core = place()
    g = 1 - core if side == 0 else core
    for rh in range(2):
        for r2 in range(group // 2):
            x = jnp.concatenate(
                [src[2 * b + rh, 16 * r2 : 16 * (r2 + 1)] for b in range(chips // 2)], axis=0
            )
            at = pl.multiple_of((g * group + rh * (group // 2) + r2) * v_dim, v_dim)
            part = dot_nn(x, w[pl.ds(at, v_dim)])
            total = part if total is None else total + part
    out[...] = total.astype(out.dtype)


def out_near_kernel(tp, src, w, out, *, group):
    out_kernel(src, None, w, out, group=group, side=0)


def out_far_kernel(tp, src, held, w, out, *, group):
    out_kernel(src, held, w, out, group=group, side=1)


def add_kernel(a, b, out):
    out[...] = (a[...].astype(F32) + b[...].astype(F32)).astype(BF16)


def on_device(
    tokens,
    norm_gain,
    query_weight,
    key_weight,
    value_weight,
    out_weight,
    head_gain,
    mix_lambda,
    cache_keys,
    cache_values,
    lengths,
    accepted,
    parents,
):
    seqs, proposals, width = tokens.shape
    n_tok = seqs * proposals
    local_kv, span = cache_keys.shape[1:3]
    group = mix_lambda.shape[0] // local_kv
    qk = cache_keys.shape[-1] // 2
    v_dim = cache_values.shape[-1]
    shards = lax.axis_size("kv")
    tps = lax.axis_size("tp")
    chips = shards // CORES
    cols = query_weight.shape[1] + key_weight.shape[1] + value_weight.shape[1]
    rows = cols // shards
    parts = chips // (2 * group)
    quarter = qk // 2 // parts
    key_rows = qk // 2 // (chips // 4)
    me = lax.axis_index("kv")
    chip, core = me // CORES, me % CORES
    same_core = [[CORES * z + c for z in range(chips)] for c in range(CORES)]
    pairs = [(i, i ^ 1) for i in range(shards)]

    block = 4
    close = [
        [CORES * (block * o + i) + c for i in range(block)]
        for o in range(chips // block)
        for c in range(CORES)
    ]
    spread = [
        [CORES * (block * o + i) + c for o in range(chips // block)]
        for i in range(block)
        for c in range(CORES)
    ]

    def over_close(x):
        x = x.reshape(block, -1, x.shape[-1])
        return lax.all_to_all(x, "kv", 0, 0, axis_index_groups=close, tiled=True)

    def over_spread(x):
        return lax.all_to_all(x, "kv", 0, 0, axis_index_groups=spread, tiled=True)

    def over_chips(x):
        return lax.all_to_all(x, "kv", 0, 0, axis_index_groups=same_core, tiled=True)

    def swap(x):
        return lax.ppermute(x, "kv", pairs)

    weights = pl.pallas_call(
        functools.partial(prep_kernel, kv_heads=local_kv, group=group, qk=qk),
        out_shape=sds((chips, cols // chips, query_weight.shape[0]), BF16),
        in_specs=[pl.BlockSpec(memory_space=pltpu.HBM)] * 3,
        out_specs=VM,
        scratch_shapes=[
            pltpu.VMEM(query_weight.shape, BF16),
            pltpu.VMEM(key_weight.shape, BF16),
            pltpu.VMEM(value_weight.shape, BF16),
            pltpu.SemaphoreType.DMA((3,)),
        ],
        compiler_params=limit(60),
        name="prep",
    )(query_weight, key_weight, value_weight)
    weights = over_close(weights)

    starts = lengths + accepted
    tok = jnp.arange(n_tok, dtype=jnp.int32)
    up = parents.reshape(n_tok) + tok // proposals * proposals
    linked = ((up[:, None] == tok[None, :]) & (tok[:, None] % proposals > 0)) | (
        tok[:, None] == tok[None, :]
    )
    blocks = 4
    normed, reach, depth = pl.pallas_call(
        norm_kernel,
        grid=(blocks,),
        out_shape=(
            sds((n_tok, width), BF16),
            sds((n_tok, n_tok), BF16),
            sds((8, n_tok), F32),
        ),
        in_specs=[
            pl.BlockSpec((n_tok // blocks, width), lambda i: (i, 0)),
            pl.BlockSpec((1, width), lambda i: (0, 0)),
            pl.BlockSpec((n_tok, n_tok), lambda i: (0, 0)),
        ],
        out_specs=(
            pl.BlockSpec((n_tok // blocks, width), lambda i: (i, 0)),
            pl.BlockSpec((n_tok, n_tok), lambda i: (0, 0)),
            pl.BlockSpec((8, n_tok), lambda i: (0, 0)),
        ),
        compiler_params=limit(16),
        name="norm",
    )(tokens.reshape(n_tok, width), norm_gain.reshape(1, width), linked.astype(BF16))
    position = jnp.repeat(starts, proposals) + depth[0].astype(jnp.int32)
    inverse = ROTARY_BASE ** (-jnp.arange(qk // 2, dtype=F32) / (qk // 2))
    angles = position.astype(F32)[None, :] * inverse[:, None]
    table = jnp.concatenate([jnp.cos(angles), jnp.sin(angles)], axis=0)
    weights, table = lax.optimization_barrier((weights, table))

    keep, send = pl.pallas_call(
        dot_kernel,
        out_shape=(sds((block * rows, n_tok), F32), sds((block * rows, n_tok), F32)),
        in_specs=[VM, VM],
        out_specs=(VM, VM),
        scratch_shapes=[pltpu.VMEM((block * rows * CORES, n_tok), F32)],
        compiler_params=limit(8),
        name="project",
    )(normed, weights)
    partial_sums = pl.pallas_call(
        gather_kernel,
        out_shape=sds((chips // block, block * rows, n_tok), F32),
        in_specs=[VM, VM],
        out_specs=VM,
        compiler_params=limit(4),
        name="halves",
    )(keep, swap(send))
    partial_sums = over_spread(partial_sums)
    projected = pl.pallas_call(
        functools.partial(rotate_kernel, quarter=quarter, key_rows=key_rows),
        out_shape=sds((block, block * rows, n_tok), BF16),
        in_specs=[VM, VM],
        out_specs=VM,
        compiler_params=limit(4),
        name="turn",
    )(partial_sums, table)
    near = over_close(projected).reshape(chips, rows, n_tok)
    far = swap(near)

    n_rows = 2 * group * proposals

    def attend(side, recv):
        return pl.pallas_call(
            functools.partial(
                attend_kernel, qk=qk, quarter=quarter, key_rows=key_rows, side=side
            ),
            in_specs=[SM, SM] + [VM] * 4,
            out_specs=(VM,) * 3,
            out_shape=(
                sds((seqs, n_rows, v_dim), BF16),
                sds((seqs, 8, n_rows), F32),
                sds((2, n_tok, v_dim), BF16),
            ),
            scratch_shapes=[pltpu.VMEM((group, n_tok, 2 * qk), BF16)],
            compiler_params=limit(16),
            cost_estimate=pl.CostEstimate(
                flops=4 * seqs * n_rows * span * v_dim,
                bytes_accessed=2 * seqs * span * v_dim * 2,
                transcendentals=seqs * n_rows * span,
            ),
            name="attend_far" if side else "attend_near",
        )(lengths, accepted, recv, reach, cache_keys, cache_values)

    acc_near, stat_near, fresh_near = attend(0, near)
    acc_in, stat_in = swap(acc_near), swap(stat_near)
    acc_far, stat_far, fresh_far = attend(1, far)
    half = group * proposals
    pieces = pl.pallas_call(
        pair_kernel,
        out_shape=sds((chips, half + 8, v_dim), BF16),
        in_specs=[VM] * 4,
        out_specs=VM,
        compiler_params=limit(8),
        name="pair",
    )(acc_far, stat_far, acc_in, stat_in)
    pieces = over_chips(pieces)
    cache_spec = pl.BlockSpec((1, local_kv, span, v_dim), lambda i: (i, 0, 0, 0))
    fresh_spec = pl.BlockSpec((2, n_tok, v_dim), lambda i: (0, 0, 0))
    keys_out, values_out = pl.pallas_call(
        store_kernel,
        grid=(seqs,),
        in_specs=[SM, SM, cache_spec, cache_spec, fresh_spec, fresh_spec],
        out_specs=(cache_spec, cache_spec),
        out_shape=(sds(cache_keys.shape, BF16), sds(cache_values.shape, BF16)),
        compiler_params=limit(16),
        cost_estimate=pl.CostEstimate(
            flops=4 * seqs * n_rows * span * v_dim,
            bytes_accessed=8 * seqs * local_kv * span * v_dim,
            transcendentals=0,
        ),
        name="store",
    )(lengths, accepted, cache_keys, cache_values, fresh_near, fresh_far)
    pieces, keys_out, values_out = lax.optimization_barrier((pieces, keys_out, values_out))
    first_head = (1 - core) * group + (chip % 2) * (group // 2)
    lam = lax.dynamic_slice_in_dim(mix_lambda, first_head, group // 2, 0)
    heads = pl.pallas_call(
        finish_kernel,
        out_shape=sds((chips, half // 2, v_dim), BF16),
        in_specs=[SM, VM, VM],
        out_specs=VM,
        compiler_params=limit(4),
        name="finish",
    )(lam, pieces, head_gain.reshape(1, v_dim))
    heads_near = over_chips(heads)
    heads_far = swap(heads_near)
    local_rows = local_kv * group * v_dim
    out_cols = out_weight.shape[1]
    heads_spec = pl.BlockSpec((chips, half // 2, v_dim), lambda i, tp: (0, 0, 0))
    weight_spec = pl.BlockSpec((local_rows, out_cols), lambda i, tp: (tp[0], 0))
    term_spec = pl.BlockSpec((n_tok, out_cols), lambda i, tp: (0, 0))

    def project_out(body, in_specs, dtype, *operands):
        return pl.pallas_call(
            functools.partial(body, group=group),
            grid_spec=pltpu.PrefetchScalarGridSpec(
                num_scalar_prefetch=1, grid=(1,), in_specs=in_specs, out_specs=term_spec
            ),
            out_shape=sds((n_tok, out_cols), dtype),
            compiler_params=limit(4),
        )(lax.axis_index("tp").reshape(1), *operands)

    partial_term = project_out(
        out_near_kernel, [heads_spec, weight_spec], F32, heads_near, out_weight
    )
    term = project_out(
        out_far_kernel,
        [heads_spec, term_spec, weight_spec],
        BF16,
        heads_far,
        partial_term,
        out_weight,
    )

    def add_from(x, hops):
        return pl.pallas_call(
            add_kernel,
            out_shape=sds(x.shape, BF16),
            in_specs=[VM] * 2,
            out_specs=VM,
            compiler_params=limit(4),
        )(x, lax.ppermute(x, "tp", hops))

    distance = 1
    while distance < tps:
        pairing = [(t, t // (2 * distance) * 2 * distance + 2 * distance - 1 - t % (2 * distance)) for t in range(tps)]
        term = add_from(term, pairing)
        distance *= 2
    mixed = term
    return (mixed.reshape(seqs, proposals, out_cols), keys_out, values_out)


def solution(mesh):
    in_specs = (
        P("grp", None, None),
        P(),
        P("kv", "tp"),
        P("kv", "tp"),
        P("kv", "tp"),
        P(None, "kv"),
        P(),
        P("tp"),
        P("grp", "tp", "kv", None),
        P("grp", "tp", "kv", None),
        P("grp"),
        P("grp"),
        P("grp", None),
    )
    out_specs = (P("grp", None, "kv"), P("grp", "tp", "kv", None), P("grp", "tp", "kv", None))
    return jax.shard_map(
        on_device, mesh=mesh, in_specs=in_specs, out_specs=out_specs, check_vma=False
    )
```

```python
import functools

import jax
import jax.numpy as jnp
from jax import lax
from jax.experimental import pallas as pl
from jax.experimental.pallas import tpu as pltpu
from jax.sharding import PartitionSpec as P


NEG_FILL = -1e30
ROTARY_BASE = 10000.0
NORM_EPS = 1e-06
CORES = 2
F32 = jnp.float32
BF16 = jnp.bfloat16
VM = pl.BlockSpec(memory_space=pltpu.VMEM)
SM = pl.BlockSpec(memory_space=pltpu.SMEM)


def limit(mib):
    return pltpu.CompilerParams(vmem_limit_bytes=mib << 20)


def sds(shape, dtype):
    return jax.ShapeDtypeStruct(shape, dtype)


def dot_nt(a, b):
    return lax.dot_general(a, b, (((1,), (1,)), ((), ())), preferred_element_type=F32)


def dot_nn(a, b):
    return lax.dot_general(a, b, (((1,), (0,)), ((), ())), preferred_element_type=F32)


def prep_kernel(wq_hbm, wk_hbm, wv_hbm, out, wq, wk, wv, sems, *, kv_heads, group, qk):
    copies = [
        pltpu.make_async_copy(src, dst, sems.at[n])
        for n, (src, dst) in enumerate([(wk_hbm, wk), (wv_hbm, wv), (wq_hbm, wq)])
    ]
    for copy in copies:
        copy.start()
    for copy in copies:
        copy.wait()
    chips = out.shape[0]
    rows = out.shape[1] // kv_heads
    parts = chips // (2 * group)
    quarter = qk // 2 // parts
    key_parts = chips // 4
    key_rows = qk // 2 // key_parts
    width = 2 * qk
    val_rows = width // (chips // 2)
    for g in range(kv_heads):
        base = rows * g
        for r in range(group):
            h = g * group + r
            t = wq[:, width * h : width * (h + 1)].astype(F32).T
            for m in range(2):
                for part in range(parts):
                    z = (r * 2 + m) * parts + part
                    lo = qk * m + quarter * part
                    hi = lo + qk // 2
                    out[z, base : base + quarter] = t[lo : lo + quarter].astype(BF16)
                    out[z, base + quarter : base + 2 * quarter] = t[hi : hi + quarter].astype(BF16)
        tk = wk[:, width * g : width * (g + 1)].astype(F32).T
        tv = wv[:, width * g : width * (g + 1)].astype(F32).T
        off = base + 2 * quarter
        for m in range(2):
            for part in range(key_parts):
                lo = qk * m + key_rows * part
                hi = lo + qk // 2
                both = jnp.concatenate([tk[lo : lo + key_rows], tk[hi : hi + key_rows]], axis=0)
                out[m * key_parts + part, off : off + 2 * key_rows] = both.astype(BF16)
        for y in range(chips // 2):
            out[chips // 2 + y, off : off + val_rows] = tv[
                val_rows * y : val_rows * (y + 1)
            ].astype(BF16)


def norm_kernel(tokens, gain, linked, normed, reach, depth):
    x = tokens[...].astype(F32)
    mean = jnp.mean(x * x, axis=-1, keepdims=True)
    normed[...] = (x * lax.rsqrt(mean + NORM_EPS) * gain[...].astype(F32)).astype(BF16)

    @pl.when(pl.program_id(0) == 0)
    def _():
        r = linked[...]
        for _ in range(5):
            r = jnp.minimum(dot_nn(r, r), 1.0).astype(BF16)
        reach[...] = r
        depth[...] = dot_nt(jnp.ones((8, r.shape[1]), BF16), r) - 1.0


def place():
    me = lax.axis_index("kv")
    return me, lax.div(me, CORES), lax.rem(me, CORES)


def dot_kernel(x, w, keep, send, scr):
    _, _, core = place()
    chips, rows, slab = w.shape
    acc = jnp.zeros((rows, x.shape[0]), F32)
    for z in range(chips):
        at = pl.multiple_of((CORES * z + core) * slab, slab)
        acc = acc + dot_nt(w[z], x[:, pl.ds(at, slab)])
    scr[...] = acc
    half = rows // CORES
    keep[...] = scr[pl.ds(pl.multiple_of(half * core, 8), half)]
    send[...] = scr[pl.ds(pl.multiple_of(half * (1 - core), 8), half)]


def rotate_kernel(keep, recv, table, out, *, quarter, key_rows):
    p = keep[...] + recv[...]
    chips = out.shape[0]
    _, chip, _ = place()
    freqs = table.shape[0] // 2
    at_q = pl.multiple_of(lax.rem(chip, freqs // quarter) * quarter, 8)
    at_k = pl.multiple_of(lax.rem(chip, freqs // key_rows) * key_rows, 8)
    cq, sq = table[pl.ds(at_q, quarter)], table[pl.ds(at_q + freqs, quarter)]
    cos_k, sin_k = table[pl.ds(at_k, key_rows)], table[pl.ds(at_k + freqs, key_rows)]
    is_key = chip < chips // 2
    ck = jnp.where(is_key, cos_k, 1.0)
    sk = jnp.where(is_key, sin_k, 0.0)
    a, c = p[:quarter], p[quarter : 2 * quarter]
    ka = p[2 * quarter : 2 * quarter + key_rows]
    kc = p[2 * quarter + key_rows :]
    turned = jnp.concatenate(
        [a * cq - c * sq, c * cq + a * sq, ka * ck - kc * sk, kc * ck + ka * sk], axis=0
    ).astype(BF16)
    for z in range(chips):
        out[z] = turned


def attend_kernel(
    lengths, accepted, recv, reach, ck, cv, acc_out, stat_out, fresh, qs, *, qk, quarter, key_rows, side
):
    kf, vf = fresh.at[0], fresh.at[1]
    chips = recv.shape[0]
    group = qs.shape[0]
    parts = chips // (2 * group)
    key_parts = chips // 4
    seqs, _, span, width = ck.shape
    n_tok = reach.shape[0]
    proposals = n_tok // seqs
    me, _, core = place()
    g = core if side == 0 else 1 - core
    scale = qk ** (-0.5)
    for r in range(group):
        pieces = []
        for m in range(2):
            v = (r * 2 + m) * parts
            pieces += [recv[v + p, 0:quarter] for p in range(parts)]
            pieces += [recv[v + p, quarter : 2 * quarter] for p in range(parts)]
        qs[r] = (jnp.concatenate(pieces, axis=0).astype(F32).T * scale).astype(BF16)
    lo = 2 * quarter
    pieces = []
    for m in range(2):
        both = [recv[m * key_parts + p, lo:].astype(F32) for p in range(key_parts)]
        pieces += [t[:key_rows] for t in both] + [t[key_rows:] for t in both]
    kf[...] = jnp.concatenate(pieces, axis=0).T.astype(BF16)
    pieces = [recv[chips // 2 + y, lo:] for y in range(chips // 2)]
    vf[...] = jnp.concatenate(pieces, axis=0).astype(F32).T.astype(BF16)

    lane = lax.broadcasted_iota(jnp.int32, (1, width), 1)
    maps = [(lane < qk).astype(F32).astype(BF16), (lane >= qk).astype(F32).astype(BF16)]
    n_rows = 2 * group * proposals
    slot = lax.rem(lax.broadcasted_iota(jnp.int32, (proposals, n_tok), 1), proposals)
    cached = lax.broadcasted_iota(jnp.int32, (1, span), 1)
    for b in range(seqs):
        row0 = b * proposals
        shift = me * span - lengths[b] - accepted[b]
        rows = []
        for rh in range(2):
            for m in range(2):
                for r2 in range(group // 2):
                    rows.append(qs[rh * (group // 2) + r2, row0 : row0 + proposals] * maps[m])
        q = jnp.concatenate(rows, axis=0)
        old = dot_nt(q, ck[b, g]) + jnp.where(cached + shift < 0, 0.0, NEG_FILL)
        at = slot - shift
        seen = (reach[row0 : row0 + proposals].astype(F32) > 0.5) & (at >= 0) & (at < span)
        new = dot_nt(q, kf[...]).reshape(2 * group, proposals, n_tok)
        new = (new + jnp.where(seen, 0.0, NEG_FILL)[None]).reshape(n_rows, n_tok)
        scores = jnp.concatenate([old, new], axis=1)
        top = jnp.max(scores, axis=1, keepdims=True)
        w = jnp.exp(scores - jnp.maximum(top, 0.5 * NEG_FILL))
        total = jnp.sum(w, axis=1, keepdims=True)
        w = w.astype(BF16)
        acc = dot_nn(w[:, :span], cv[b, g]) + dot_nn(w[:, span:], vf[...])
        acc_out[b] = acc.astype(BF16)
        lanes = lax.broadcasted_iota(jnp.int32, (n_rows, 128), 1)
        stat = jnp.where(lanes == 0, top, jnp.where(lanes == 1, total, 0.0))
        stat_out[b] = stat.T[:8]


def store_kernel(lengths, accepted, ck, cv, fresh_near, fresh_far, ko, vo):
    me, _, core = place()
    b = pl.program_id(0)
    heads, span, width = ck.shape[1:]
    n_tok = fresh_near.shape[1]
    proposals = n_tok // pl.num_programs(0)
    shift = me * span - lengths[b] - accepted[b]
    ko[...] = ck[...]
    vo[...] = cv[...]

    @pl.when((shift < proposals) & (shift + span > 0))
    def _():
        rel = lax.broadcasted_iota(jnp.int32, (span, n_tok), 0) + shift
        col = lax.broadcasted_iota(jnp.int32, (span, n_tok), 1) - b * proposals
        inside = (rel >= 0) & (rel < proposals)
        onehot = jnp.where(inside & (rel == col), 1.0, 0.0).astype(BF16)
        rel = lax.broadcasted_iota(jnp.int32, (span, width), 0) + shift
        written = (rel >= 0) & (rel < proposals)
        for g in range(heads):
            near = jnp.where(core == g, 1.0, 0.0)
            for n, (old, new) in enumerate(((ck, ko), (cv, vo))):
                fresh = fresh_near[n].astype(F32) * near + fresh_far[n].astype(F32) * (1.0 - near)
                placed = dot_nn(onehot, fresh.astype(BF16))
                new[0, g] = jnp.where(written, placed, old[0, g].astype(F32)).astype(BF16)


def split3(x):
    hi = x.astype(BF16).astype(F32)
    mid = (x - hi).astype(BF16).astype(F32)
    lo = (x - hi - mid).astype(BF16).astype(F32)
    return [hi, mid, lo]


def pair_kernel(acc0, stat0, acc1, stat1, out):
    seqs, rows, _ = acc0.shape
    half = rows // 2
    for b in range(seqs):
        t0, n0 = stat0[b, 0:1], stat0[b, 1:2]
        t1, n1 = stat1[b, 0:1], stat1[b, 1:2]
        top = jnp.maximum(t0, t1)
        e0, e1 = jnp.exp(t0 - top), jnp.exp(t1 - top)
        total = n0 * e0 + n1 * e1
        cols = jnp.concatenate([e0, e1, jnp.zeros((6, rows), F32)], axis=0).T
        acc = acc0[b].astype(F32) * cols[:, 0:1] + acc1[b].astype(F32) * cols[:, 1:2]
        acc = acc.astype(BF16)
        info = jnp.concatenate(split3(top) + split3(total) + [jnp.zeros((2, rows), F32)], axis=0)
        for rh in range(2):
            out[2 * b + rh, 0:half] = acc[half * rh : half * (rh + 1)]
            view = info if rh == 0 else pltpu.roll(info, half, 1)
            out[2 * b + rh, half : half + 8] = view.astype(BF16)


def finish_kernel(lam, recv, gain, out):
    chips, full, _ = recv.shape
    half = full - 8
    tops, totals = [], []
    for s in range(chips):
        info = recv[s, half:].astype(F32)
        tops.append(info[0:1] + info[1:2] + info[2:3])
        totals.append(info[3:4] + info[4:5] + info[5:6])
    tops = jnp.concatenate(tops, axis=0)
    totals = jnp.concatenate(totals, axis=0)
    scale = jnp.exp(tops - jnp.max(tops, axis=0, keepdims=True))
    den = jnp.sum(scale * totals, axis=0, keepdims=True)
    cols = jnp.concatenate([scale, den, jnp.zeros((7, scale.shape[1]), F32)], axis=0).T[:half]
    num = recv[0, 0:half].astype(F32) * cols[:, 0:1]
    for s in range(1, chips):
        num = num + recv[s, 0:half].astype(F32) * cols[:, s : s + 1]
    attended = num / cols[:, chips : chips + 1]
    quarter = half // 2
    row = lax.broadcasted_iota(jnp.int32, (quarter, 1), 0)
    lam_col = jnp.where(row < quarter // 2, lam[0], lam[1])
    diff = attended[:quarter] - lam_col * attended[quarter:]
    mean = jnp.mean(diff * diff, axis=-1, keepdims=True)
    res = (diff * lax.rsqrt(mean + NORM_EPS) * gain[...].astype(F32)).astype(BF16)
    for z in range(chips):
        out[z] = res


def out_kernel(src, held, w, out, *, group, side):
    chips, _, v_dim = src.shape
    total = held[...] if held is not None else None
    _, _, core = place()
    g = 1 - core if side == 0 else core
    for rh in range(2):
        for r2 in range(group // 2):
            x = jnp.concatenate(
                [src[2 * b + rh, 16 * r2 : 16 * (r2 + 1)] for b in range(chips // 2)], axis=0
            )
            at = pl.multiple_of((g * group + rh * (group // 2) + r2) * v_dim, v_dim)
            part = dot_nn(x, w[pl.ds(at, v_dim)])
            total = part if total is None else total + part
    out[...] = total.astype(out.dtype)


def out_near_kernel(tp, src, w, out, *, group):
    out_kernel(src, None, w, out, group=group, side=0)


def out_far_kernel(tp, src, held, w, out, *, group):
    out_kernel(src, held, w, out, group=group, side=1)


def add_kernel(a, b, out):
    out[...] = (a[...].astype(F32) + b[...].astype(F32)).astype(BF16)


def on_device(
    tokens,
    norm_gain,
    query_weight,
    key_weight,
    value_weight,
    out_weight,
    head_gain,
    mix_lambda,
    cache_keys,
    cache_values,
    lengths,
    accepted,
    parents,
):
    seqs, proposals, width = tokens.shape
    n_tok = seqs * proposals
    local_kv, span = cache_keys.shape[1:3]
    group = mix_lambda.shape[0] // local_kv
    qk = cache_keys.shape[-1] // 2
    v_dim = cache_values.shape[-1]
    shards = lax.axis_size("kv")
    tps = lax.axis_size("tp")
    chips = shards // CORES
    cols = query_weight.shape[1] + key_weight.shape[1] + value_weight.shape[1]
    rows = cols // shards
    parts = chips // (2 * group)
    quarter = qk // 2 // parts
    key_rows = qk // 2 // (chips // 4)
    me = lax.axis_index("kv")
    chip, core = me // CORES, me % CORES
    same_core = [[CORES * z + c for z in range(chips)] for c in range(CORES)]
    pairs = [(i, i ^ 1) for i in range(shards)]

    def over_chips(x):
        return lax.all_to_all(x, "kv", 0, 0, axis_index_groups=same_core, tiled=True)

    def swap(x):
        return lax.ppermute(x, "kv", pairs)

    weights = pl.pallas_call(
        functools.partial(prep_kernel, kv_heads=local_kv, group=group, qk=qk),
        out_shape=sds((chips, cols // chips, query_weight.shape[0]), BF16),
        in_specs=[pl.BlockSpec(memory_space=pltpu.HBM)] * 3,
        out_specs=VM,
        scratch_shapes=[
            pltpu.VMEM(query_weight.shape, BF16),
            pltpu.VMEM(key_weight.shape, BF16),
            pltpu.VMEM(value_weight.shape, BF16),
            pltpu.SemaphoreType.DMA((3,)),
        ],
        compiler_params=limit(60),
        name="prep",
    )(query_weight, key_weight, value_weight)
    weights = over_chips(weights)

    starts = lengths + accepted
    tok = jnp.arange(n_tok, dtype=jnp.int32)
    up = parents.reshape(n_tok) + tok // proposals * proposals
    linked = ((up[:, None] == tok[None, :]) & (tok[:, None] % proposals > 0)) | (
        tok[:, None] == tok[None, :]
    )
    blocks = 4
    normed, reach, depth = pl.pallas_call(
        norm_kernel,
        grid=(blocks,),
        out_shape=(
            sds((n_tok, width), BF16),
            sds((n_tok, n_tok), BF16),
            sds((8, n_tok), F32),
        ),
        in_specs=[
            pl.BlockSpec((n_tok // blocks, width), lambda i: (i, 0)),
            pl.BlockSpec((1, width), lambda i: (0, 0)),
            pl.BlockSpec((n_tok, n_tok), lambda i: (0, 0)),
        ],
        out_specs=(
            pl.BlockSpec((n_tok // blocks, width), lambda i: (i, 0)),
            pl.BlockSpec((n_tok, n_tok), lambda i: (0, 0)),
            pl.BlockSpec((8, n_tok), lambda i: (0, 0)),
        ),
        compiler_params=limit(16),
        name="norm",
    )(tokens.reshape(n_tok, width), norm_gain.reshape(1, width), linked.astype(BF16))
    position = jnp.repeat(starts, proposals) + depth[0].astype(jnp.int32)
    inverse = ROTARY_BASE ** (-jnp.arange(qk // 2, dtype=F32) / (qk // 2))
    angles = position.astype(F32)[None, :] * inverse[:, None]
    table = jnp.concatenate([jnp.cos(angles), jnp.sin(angles)], axis=0)
    weights, table = lax.optimization_barrier((weights, table))

    keep, send = pl.pallas_call(
        dot_kernel,
        out_shape=(sds((rows, n_tok), F32), sds((rows, n_tok), F32)),
        in_specs=[VM, VM],
        out_specs=(VM, VM),
        scratch_shapes=[pltpu.VMEM((rows * CORES, n_tok), F32)],
        compiler_params=limit(8),
        name="project",
    )(normed, weights)
    projected = pl.pallas_call(
        functools.partial(rotate_kernel, quarter=quarter, key_rows=key_rows),
        out_shape=sds((chips, rows, n_tok), BF16),
        in_specs=[VM, VM, VM],
        out_specs=VM,
        compiler_params=limit(4),
        name="turn",
    )(keep, swap(send), table)
    near = over_chips(projected)
    far = swap(near)

    n_rows = 2 * group * proposals

    def attend(side, recv):
        return pl.pallas_call(
            functools.partial(
                attend_kernel, qk=qk, quarter=quarter, key_rows=key_rows, side=side
            ),
            in_specs=[SM, SM] + [VM] * 4,
            out_specs=(VM,) * 3,
            out_shape=(
                sds((seqs, n_rows, v_dim), BF16),
                sds((seqs, 8, n_rows), F32),
                sds((2, n_tok, v_dim), BF16),
            ),
            scratch_shapes=[pltpu.VMEM((group, n_tok, 2 * qk), BF16)],
            compiler_params=limit(16),
            cost_estimate=pl.CostEstimate(
                flops=4 * seqs * n_rows * span * v_dim,
                bytes_accessed=2 * seqs * span * v_dim * 2,
                transcendentals=seqs * n_rows * span,
            ),
            name="attend_far" if side else "attend_near",
        )(lengths, accepted, recv, reach, cache_keys, cache_values)

    acc_near, stat_near, fresh_near = attend(0, near)
    acc_in, stat_in = swap(acc_near), swap(stat_near)
    acc_far, stat_far, fresh_far = attend(1, far)
    half = group * proposals
    pieces = pl.pallas_call(
        pair_kernel,
        out_shape=sds((chips, half + 8, v_dim), BF16),
        in_specs=[VM] * 4,
        out_specs=VM,
        compiler_params=limit(8),
        name="pair",
    )(acc_far, stat_far, acc_in, stat_in)
    pieces = over_chips(pieces)
    cache_spec = pl.BlockSpec((1, local_kv, span, v_dim), lambda i: (i, 0, 0, 0))
    fresh_spec = pl.BlockSpec((2, n_tok, v_dim), lambda i: (0, 0, 0))
    keys_out, values_out = pl.pallas_call(
        store_kernel,
        grid=(seqs,),
        in_specs=[SM, SM, cache_spec, cache_spec, fresh_spec, fresh_spec],
        out_specs=(cache_spec, cache_spec),
        out_shape=(sds(cache_keys.shape, BF16), sds(cache_values.shape, BF16)),
        compiler_params=limit(16),
        cost_estimate=pl.CostEstimate(
            flops=4 * seqs * n_rows * span * v_dim,
            bytes_accessed=8 * seqs * local_kv * span * v_dim,
            transcendentals=0,
        ),
        name="store",
    )(lengths, accepted, cache_keys, cache_values, fresh_near, fresh_far)
    pieces, keys_out, values_out = lax.optimization_barrier((pieces, keys_out, values_out))
    first_head = (1 - core) * group + (chip % 2) * (group // 2)
    lam = lax.dynamic_slice_in_dim(mix_lambda, first_head, group // 2, 0)
    heads = pl.pallas_call(
        finish_kernel,
        out_shape=sds((chips, half // 2, v_dim), BF16),
        in_specs=[SM, VM, VM],
        out_specs=VM,
        compiler_params=limit(4),
        name="finish",
    )(lam, pieces, head_gain.reshape(1, v_dim))
    heads_near = over_chips(heads)
    heads_far = swap(heads_near)
    local_rows = local_kv * group * v_dim
    out_cols = out_weight.shape[1]
    heads_spec = pl.BlockSpec((chips, half // 2, v_dim), lambda i, tp: (0, 0, 0))
    weight_spec = pl.BlockSpec((local_rows, out_cols), lambda i, tp: (tp[0], 0))
    term_spec = pl.BlockSpec((n_tok, out_cols), lambda i, tp: (0, 0))

    def project_out(body, in_specs, dtype, *operands):
        return pl.pallas_call(
            functools.partial(body, group=group),
            grid_spec=pltpu.PrefetchScalarGridSpec(
                num_scalar_prefetch=1, grid=(1,), in_specs=in_specs, out_specs=term_spec
            ),
            out_shape=sds((n_tok, out_cols), dtype),
            compiler_params=limit(4),
        )(lax.axis_index("tp").reshape(1), *operands)

    partial_term = project_out(
        out_near_kernel, [heads_spec, weight_spec], F32, heads_near, out_weight
    )
    term = project_out(
        out_far_kernel,
        [heads_spec, term_spec, weight_spec],
        BF16,
        heads_far,
        partial_term,
        out_weight,
    )

    def add_from(x, hops):
        return pl.pallas_call(
            add_kernel,
            out_shape=sds(x.shape, BF16),
            in_specs=[VM] * 2,
            out_specs=VM,
            compiler_params=limit(4),
        )(x, lax.ppermute(x, "tp", hops))

    distance = 1
    while distance < tps:
        pairing = [(t, t // (2 * distance) * 2 * distance + 2 * distance - 1 - t % (2 * distance)) for t in range(tps)]
        term = add_from(term, pairing)
        distance *= 2
    mixed = term
    return (mixed.reshape(seqs, proposals, out_cols), keys_out, values_out)


def solution(mesh):
    in_specs = (
        P("grp", None, None),
        P(),
        P("kv", "tp"),
        P("kv", "tp"),
        P("kv", "tp"),
        P(None, "kv"),
        P(),
        P("tp"),
        P("grp", "tp", "kv", None),
        P("grp", "tp", "kv", None),
        P("grp"),
        P("grp"),
        P("grp", None),
    )
    out_specs = (P("grp", None, "kv"), P("grp", "tp", "kv", None), P("grp", "tp", "kv", None))
    return jax.shard_map(
        on_device, mesh=mesh, in_specs=in_specs, out_specs=out_specs, check_vma=False
    )
```
